32 devices in a mesh: sp: 8 (over z, y), tp: 4 (over x, core).
Axes of the slice: x: 2, y: 2, z: 4, core: 2. Of those that a mesh axis runs over, the one named last changes fastest.
Arguments:
- queries: bfloat16 [6144, 1024], P('sp', 'tp'), may hold values from -8 to 8
- keys: bfloat16 [6144, 256], P('sp', 'tp'), may hold values from -8 to 8
- values: bfloat16 [6144, 256], P('sp', 'tp'), may hold values from -18 to 18
- query_gain: float32 [64], replicated, may hold values from 0.4 to 5.5
- key_gain: float32 [64], replicated, may hold values from 0.4 to 5.5
- sink_logits: float32 [16], P('tp'), may hold values from 2 to 5
- out_weight: bfloat16 [1024, 2048], P('tp'), may hold values from -0.1875 to 0.1875
- residual: bfloat16 [6144, 2048], P('sp', 'tp'), may hold values from -21 to 21
- norm_gain: float32 [2048], P('tp'), may hold values from 0.1 to 1.9
- gate_weight: bfloat16 [2048, 5632], P('sp', 'tp'), may hold values from -0.125 to 0.125
- up_weight: bfloat16 [2048, 5632], P('sp', 'tp'), may hold values from -0.125 to 0.125
- down_weight: bfloat16 [5632, 2048], P('tp', 'sp'), may hold values from -0.078125 to 0.078125
Outputs:
- layer_out: bfloat16 [6144, 2048], P('sp', 'tp')
The draws below stay inside these ranges and needn't reach their ends.
All inputs are finite; a program needn't handle non-finite values.
Results may differ from the reference program's by a relative error of at most 0.0095.
The reference program's roundings to bfloat16 on the way count: a program that leaves them out, or rounds other values in their place, can miss the bound.
Values may be sent and summed in bfloat16 or wider, within the bound.
No kernel may reach another device: no remote copies, remote signals or barrier semaphores. Data moves between devices by JAX's collectives and lax.ppermute only.
A program may use at most 192 MiB of HBM per device.

```python
import jax
import jax.numpy as jnp
from jax import lax

D = 2048
FF = 5632
HEAD_DIM = 64
Q_HEADS = 16
KV_HEADS = 4
WINDOW = 128
TOKENS = 6144
N_TP = 4


def shared_fields(key):
    key_rows = jnp.clip(jax.random.normal(jax.random.fold_in(key, 101), (TOKENS, KV_HEADS * HEAD_DIM), jnp.float32), -6.0, 6.0)
    query_rows = jnp.clip(jax.random.normal(jax.random.fold_in(key, 102), (TOKENS, Q_HEADS * HEAD_DIM), jnp.float32), -6.0, 6.0)
    return (key_rows, query_rows)


def draw_keys(key, part):
    return shared_fields(key)[0].astype(jnp.bfloat16)


def draw_queries(key, part):
    return shared_fields(key)[1].astype(jnp.bfloat16)


def gain_draw(key):
    return 1.0 + 0.18 * jnp.clip(jax.random.normal(key, (HEAD_DIM,), jnp.float32), -3.0, 3.0)


def draw_query_gain(key, part):
    return gain_draw(jax.random.fold_in(key, 104))


def draw_key_gain(key, part):
    return gain_draw(jax.random.fold_in(key, 105))


def draw_residual(key, part):
    columns = jnp.arange(D).astype(jnp.float32)
    col_scale = 3.0 ** (columns / (D - 1))
    base = jnp.clip(jax.random.normal(jax.random.fold_in(key, 106), (TOKENS, D), jnp.float32), -6.0, 6.0)
    return (base * col_scale).astype(jnp.bfloat16)


def shard_levels(own_key, shape, pieces, low, top_value):
    factor_of, own = 1.0, jax.random.fold_in(own_key, 6)
    for dim, blocks in pieces:
        steps = jnp.exp(jax.random.uniform(jax.random.fold_in(own, dim), (blocks,), jnp.float32, low / len(pieces), top_value / len(pieces)))
        factor_of = factor_of * jnp.repeat(steps, shape[dim] // blocks).reshape([-1 if axis == dim else 1 for axis in range(len(shape))])
    return factor_of


def bell_draw(own_key, extent, scale, reach, pieces=(), kind=jnp.bfloat16):
    result = jax.random.normal(own_key, extent, jnp.float32) * scale
    if len(pieces) > 0:
        result = shard_levels(own_key, extent, pieces, -0.22, 0.18) * result
    return jnp.clip(result, min=-reach, max=reach).astype(kind)


def setup_inputs(seed: int = 0) -> dict:
    splits = jax.random.split(jax.random.key(seed), 13)
    return {
        "queries": draw_queries(jax.random.fold_in(splits[12], 71), 0),
        "keys": draw_keys(jax.random.fold_in(splits[12], 71), 0),
        "values": bell_draw(splits[2], (TOKENS, KV_HEADS * HEAD_DIM), 3.0, 18.0, ((0, 8), (1, 4))),
        "query_gain": draw_query_gain(jax.random.fold_in(splits[12], 71), 0),
        "key_gain": draw_key_gain(jax.random.fold_in(splits[12], 71), 0),
        "sink_logits": jnp.clip(2.0 + 3.0 * jax.random.uniform(splits[5], (Q_HEADS,), jnp.float32) ** shard_levels(splits[5], (Q_HEADS,), ((0, 4),), -0.2, 0.2), 2.0, 5.0),
        "out_weight": bell_draw(splits[6], (Q_HEADS * HEAD_DIM, D), (Q_HEADS * HEAD_DIM) ** -0.5, 0.1875, ((0, 4),)),
        "residual": draw_residual(jax.random.fold_in(splits[12], 71), 0),
        "norm_gain": jnp.clip(1.0 + 0.18 * jax.random.normal(splits[8], (D,), jnp.float32), 0.1, 1.9),
        "gate_weight": bell_draw(splits[9], (D, FF), D ** -0.5, 0.125, ((0, 8), (1, 4))),
        "up_weight": bell_draw(splits[10], (D, FF), D ** -0.5, 0.125, ((0, 8), (1, 4))),
        "down_weight": bell_draw(splits[11], (FF, D), FF ** -0.5, 0.078125, ((0, 4), (1, 8))),
    }


def norm_heads(flat, gain, heads):
    row_count = flat.shape[0]
    head_width = gain.shape[0]
    data = flat.astype(jnp.float32).reshape(row_count, heads, head_width)
    scaled = data * lax.rsqrt(lax.optimization_barrier(jnp.mean(data * data, axis=-1, keepdims=True)) + 1e-06) * gain
    return scaled.astype(jnp.bfloat16)

def reference(queries, keys, values, query_gain, key_gain, sink_logits, out_weight, residual, norm_gain, gate_weight, up_weight, down_weight):
    seq_len = queries.shape[0]
    group_size = Q_HEADS // KV_HEADS
    block_count = seq_len // WINDOW
    query_heads = norm_heads(queries, query_gain, Q_HEADS).reshape(seq_len, KV_HEADS, group_size, HEAD_DIM).transpose(1, 0, 2, 3)
    key_heads = norm_heads(keys, key_gain, KV_HEADS).transpose(1, 0, 2)
    value_heads = values.reshape(seq_len, KV_HEADS, HEAD_DIM).transpose(1, 0, 2)
    sink_rows = sink_logits.reshape(KV_HEADS, group_size)
    query_index = jnp.arange(WINDOW)[:, None]
    key_index = jnp.arange(2 * WINDOW)[None, :]
    offset_lag = WINDOW + query_index - key_index
    inband = (offset_lag >= 0) & (offset_lag < WINDOW)
    leading = (jnp.arange(block_count)[:, None, None] > 0) | (key_index[None] >= WINDOW)
    valid = inband[None] & leading

    def one_head(operands):
        query_h, key_h, value_h, sink_h = operands
        zero_rows = jnp.zeros((WINDOW, HEAD_DIM), jnp.bfloat16)
        key_prev = jnp.concatenate([zero_rows, key_h[:seq_len - WINDOW]], axis=0)
        value_prev = jnp.concatenate([zero_rows, value_h[:seq_len - WINDOW]], axis=0)
        key_blocks = jnp.concatenate([key_prev.reshape(block_count, WINDOW, HEAD_DIM), key_h.reshape(block_count, WINDOW, HEAD_DIM)], axis=1).astype(jnp.float32)
        value_blocks = jnp.concatenate([value_prev.reshape(block_count, WINDOW, HEAD_DIM), value_h.reshape(block_count, WINDOW, HEAD_DIM)], axis=1).astype(jnp.float32)
        query_blocks = query_h.reshape(block_count, WINDOW, group_size, HEAD_DIM).astype(jnp.float32)
        scores = jnp.einsum('nqgd,nkd->ngqk', query_blocks, key_blocks) * HEAD_DIM ** (-0.5)
        scores = jnp.where(valid[:, None], scores, -1e+30)
        sink_b = sink_h[None, :, None]
        row_peak = jnp.maximum(lax.optimization_barrier(jnp.max(scores, axis=-1)), sink_b)
        exp_terms = jnp.exp(scores - row_peak[..., None])
        denom_sum = lax.optimization_barrier(jnp.sum(exp_terms, axis=-1)) + jnp.exp(sink_b - row_peak)
        weights = (exp_terms / denom_sum[..., None]).astype(jnp.bfloat16)
        attended = jnp.einsum('ngqk,nkd->nqgd', weights.astype(jnp.float32), value_blocks).astype(jnp.bfloat16)
        return attended.reshape(seq_len, group_size, HEAD_DIM)
    heads_out = lax.map(one_head, (query_heads, key_heads, value_heads, sink_rows))
    attended = heads_out.transpose(1, 0, 2, 3).reshape(seq_len, Q_HEADS * HEAD_DIM)
    slice_width = Q_HEADS * HEAD_DIM // N_TP
    mixed = jnp.zeros((seq_len, D), jnp.float32)
    for member in range(N_TP):
        lower = member * slice_width
        product = jnp.dot(attended[:, lower:lower + slice_width], out_weight[lower:lower + slice_width], preferred_element_type=jnp.float32)
        mixed = mixed + product.astype(jnp.bfloat16).astype(jnp.float32)
    middle = (residual.astype(jnp.float32) + mixed).astype(jnp.bfloat16)
    middle_wide = middle.astype(jnp.float32)
    normed = (middle_wide * lax.rsqrt(lax.optimization_barrier(jnp.mean(middle_wide * middle_wide, axis=1, keepdims=True)) + 1e-06) * norm_gain).astype(jnp.bfloat16)
    hidden_width = FF // N_TP
    feed = jnp.zeros((seq_len, D), jnp.float32)
    for member in range(N_TP):
        lower = member * hidden_width
        gate_acts = jnp.dot(normed, gate_weight[:, lower:lower + hidden_width], preferred_element_type=jnp.float32)
        up_acts = jnp.dot(normed, up_weight[:, lower:lower + hidden_width], preferred_element_type=jnp.float32)
        hidden = (jax.nn.silu(gate_acts) * up_acts).astype(jnp.bfloat16)
        product = jnp.dot(hidden, down_weight[lower:lower + hidden_width], preferred_element_type=jnp.float32)
        feed = feed + product.astype(jnp.bfloat16).astype(jnp.float32)
    return (middle_wide + 0.5 * feed).astype(jnp.bfloat16)
```

```python
import functools

import jax
import jax.numpy as jnp
from jax import lax
from jax.experimental import pallas as pl
from jax.experimental.pallas import tpu as pltpu
from jax.sharding import Mesh
from jax.sharding import PartitionSpec as P

WINDOW = 128
EPS = 1e-06
LANES = 128


def from_behind(block, axes, count):
    return lax.ppermute(block, axes, [(i - 1, i) for i in range(1, count)])


def norm_heads(flat, gain, heads):
    row_count = flat.shape[0]
    head_width = gain.shape[0]
    data = flat.astype(jnp.float32).reshape(row_count, heads, head_width)
    scaled = data * lax.rsqrt(jnp.mean(data * data, axis=-1, keepdims=True) + EPS) * gain
    return scaled.astype(jnp.bfloat16)


def attention(queries, keys, values, query_gain, key_gain, sink_logits, sp_axes, sp_count):
    head_width = query_gain.shape[0]
    row_count = queries.shape[0]
    q_heads = queries.shape[1] // head_width
    k_heads = keys.shape[1] // head_width
    group_size = q_heads // k_heads
    window_len = WINDOW
    block_count = row_count // window_len
    kv_width = k_heads * head_width
    query_norm = norm_heads(queries, query_gain, q_heads)
    key_norm = norm_heads(keys, key_gain, k_heads).reshape(row_count, kv_width)
    tail = jnp.concatenate(
        [key_norm[row_count - window_len :], values[row_count - window_len :]], axis=1
    )
    prev = from_behind(tail, sp_axes, sp_count)
    prev_keys, prev_values = prev[:, :kv_width], prev[:, kv_width:]
    key_all = jnp.concatenate([prev_keys, key_norm], axis=0)
    value_all = jnp.concatenate([prev_values, values], axis=0)

    def blocks(whole, own):
        return jnp.concatenate(
            [
                whole[:row_count].reshape(block_count, window_len, k_heads, head_width),
                own.reshape(block_count, window_len, k_heads, head_width),
            ],
            axis=1,
        )

    key_blocks = blocks(key_all, key_norm)
    value_blocks = blocks(value_all, values)
    query_blocks = query_norm.reshape(block_count, window_len, k_heads, group_size, head_width)
    scores = jnp.einsum(
        "nqhgd,nkhd->nhgqk", query_blocks, key_blocks, preferred_element_type=jnp.float32
    ) * head_width ** (-0.5)
    query_index = jnp.arange(window_len)[:, None]
    key_index = jnp.arange(2 * window_len)[None, :]
    offset_lag = window_len + query_index - key_index
    inband = (offset_lag >= 0) & (offset_lag < window_len)
    leading = (
        (jnp.arange(block_count)[:, None, None] > 0)
        | (key_index[None] >= window_len)
        | (lax.axis_index(sp_axes) > 0)
    )
    valid = inband[None] & leading
    scores = jnp.where(valid[:, None, None], scores, -1e30)
    sink_rows = sink_logits.reshape(k_heads, group_size)[None, :, :, None]
    row_peak = jnp.maximum(jnp.max(scores, axis=-1), sink_rows)
    exp_terms = jnp.exp(scores - row_peak[..., None])
    denom_sum = jnp.sum(exp_terms, axis=-1) + jnp.exp(sink_rows - row_peak)
    weights = (exp_terms / denom_sum[..., None]).astype(jnp.bfloat16)
    attended = jnp.einsum(
        "nhgqk,nkhd->nqhgd", weights, value_blocks, preferred_element_type=jnp.float32
    ).astype(jnp.bfloat16)
    return attended.reshape(row_count, q_heads * head_width)


def general_device(model_width, *args):
    (queries, keys, values, query_gain, key_gain, sink_logits, out_weight, residual) = args[:8]
    (norm_gain, gate_weight, up_weight, down_weight) = args[8:]
    gate_full = lax.all_gather(gate_weight, "sp", axis=0, tiled=True)
    up_full = lax.all_gather(up_weight, "sp", axis=0, tiled=True)
    down_full = lax.all_gather(down_weight, "sp", axis=1, tiled=True)
    attended = attention(
        queries, keys, values, query_gain, key_gain, sink_logits, "sp", lax.axis_size("sp")
    )
    projected = jnp.dot(attended, out_weight, preferred_element_type=jnp.float32)
    mixed = lax.psum_scatter(
        projected.astype(jnp.bfloat16), "tp", scatter_dimension=1, tiled=True
    ).astype(jnp.float32)
    middle_wide = (residual.astype(jnp.float32) + mixed).astype(jnp.bfloat16).astype(jnp.float32)
    squares = lax.psum(jnp.sum(middle_wide * middle_wide, axis=1), "tp")
    scale = lax.rsqrt(squares / model_width + EPS)[:, None]
    normed = (middle_wide * scale * norm_gain).astype(jnp.bfloat16)
    normed_all = lax.all_gather(normed, "tp", axis=1, tiled=True)
    gate_acts = jnp.dot(normed_all, gate_full, preferred_element_type=jnp.float32)
    up_acts = jnp.dot(normed_all, up_full, preferred_element_type=jnp.float32)
    hidden = (jax.nn.silu(gate_acts) * up_acts).astype(jnp.bfloat16)
    down_terms = jnp.dot(hidden, down_full, preferred_element_type=jnp.float32)
    summed_back = lax.psum_scatter(
        down_terms.astype(jnp.bfloat16), "tp", scatter_dimension=1, tiled=True
    ).astype(jnp.float32)
    return (middle_wide + 0.5 * summed_back).astype(jnp.bfloat16)


def swap(block, axis):
    return lax.ppermute(block, axis, [(0, 1), (1, 0)])


def project_kernel(
    place_ref, att_ref, att_c_ref, out_w_ref, out_wc_ref, res_ref, res_c_ref, gain_ref,
    normed_ref, middle_ref, acc,
):
    width = res_ref.shape[1] // 2
    acc[...] = jnp.dot(att_ref[...], out_w_ref[...], preferred_element_type=jnp.float32)
    acc[...] += jnp.dot(att_c_ref[...], out_wc_ref[...], preferred_element_type=jnp.float32)
    for n, ref in enumerate((res_ref, res_ref, res_c_ref, res_c_ref)):
        columns = pl.ds(pl.multiple_of(place_ref[n] * width, width), width)
        half = slice((n % 2) * width, (n % 2 + 1) * width)
        acc[:, columns] += ref[:, half].astype(jnp.float32)
    middle = acc[...].astype(jnp.bfloat16)
    wide = middle.astype(jnp.float32)
    acc[...] = wide
    scale = lax.rsqrt(jnp.mean(wide * wide, axis=1, keepdims=True) + EPS)
    normed_ref[...] = (wide * scale * gain_ref[...]).astype(jnp.bfloat16)
    own = pl.ds(pl.multiple_of(place_ref[0] * width, width), width)
    middle_ref[...] = acc[:, own].astype(jnp.bfloat16)


def project(place, att, att_c, out_w, out_wc, res, res_c, gain, tile):
    rows, depth = att.shape
    width = out_w.shape[1]
    part = res.shape[1]
    row_spec = lambda n: pl.BlockSpec((tile, n), lambda i, p: (i, 0))
    full_spec = lambda a: pl.BlockSpec(a.shape, lambda i, p: (0, 0))
    return pl.pallas_call(
        project_kernel,
        grid_spec=pltpu.PrefetchScalarGridSpec(
            num_scalar_prefetch=1,
            grid=(rows // tile,),
            in_specs=[
                row_spec(depth), row_spec(depth), full_spec(out_w), full_spec(out_wc),
                row_spec(part), row_spec(part), full_spec(gain),
            ],
            out_specs=[row_spec(width), row_spec(part // 2)],
            scratch_shapes=[pltpu.VMEM((tile, width), jnp.float32)],
        ),
        out_shape=[
            jax.ShapeDtypeStruct((rows, width), jnp.bfloat16),
            jax.ShapeDtypeStruct((rows, part // 2), jnp.bfloat16),
        ],
        compiler_params=pltpu.CompilerParams(vmem_limit_bytes=48 * 2**20),
        cost_estimate=pl.CostEstimate(
            flops=4 * rows * depth * width, bytes_accessed=4 * rows * width, transcendentals=0
        ),
        name="project",
    )(place, att, att_c, out_w, out_wc, res, res_c, gain)


def hidden_kernel(main, tail, count, place_ref, x_ref, *refs):
    pieces, out_ref, whole = refs[:count], refs[count], refs[count + 1]
    depth = pieces[0].shape[0]

    @pl.when(pl.program_id(0) == 0)
    def _():
        for n, piece in enumerate(pieces):
            rows = pl.ds(pl.multiple_of(place_ref[n] * depth, depth), depth)
            whole[rows, :] = piece[...]

    acts = jnp.dot(x_ref[...], whole[...], preferred_element_type=jnp.float32)

    def gated(gate, up):
        return (gate / (1.0 + jnp.exp(-gate)) * up).astype(jnp.bfloat16)

    out_ref[:, :main] = gated(acts[:, :main], acts[:, main : 2 * main])
    if tail:
        rest = acts[:, 2 * main :]
        out_ref[:, main:] = gated(rest[:, :tail], rest[:, tail:])


def hidden_units(place, x, pieces, main, tail, tile):
    rows, depth = x.shape
    width = pieces[0].shape[1]
    return pl.pallas_call(
        functools.partial(hidden_kernel, main, tail, len(pieces)),
        grid_spec=pltpu.PrefetchScalarGridSpec(
            num_scalar_prefetch=1,
            grid=(rows // tile,),
            in_specs=[pl.BlockSpec((tile, depth), lambda i, p: (i, 0))]
            + [pl.BlockSpec(p.shape, lambda i, p: (0, 0)) for p in pieces],
            out_specs=pl.BlockSpec((tile, main + tail), lambda i, p: (i, 0)),
            scratch_shapes=[pltpu.VMEM((depth, width), jnp.bfloat16)],
        ),
        out_shape=jax.ShapeDtypeStruct((rows, main + tail), jnp.bfloat16),
        compiler_params=pltpu.CompilerParams(vmem_limit_bytes=48 * 2**20),
        cost_estimate=pl.CostEstimate(
            flops=2 * rows * depth * width, bytes_accessed=2 * rows * depth, transcendentals=0
        ),
        name="hidden_units",
    )(place, x, *pieces)


def paired_device(
    queries, keys, values, query_gain, key_gain, sink_logits, out_weight, residual, norm_gain,
    gate_weight, up_weight, down_weight,
):
    zh, zl, y, x, c = (lax.axis_index(a) for a in ("zh", "zl", "y", "x", "c"))
    rows = queries.shape[0]
    block = down_weight.shape[1]
    units = gate_weight.shape[1]
    main = units // LANES // 2 * LANES
    tail = (units - 2 * main) // 2
    low = zl == 0

    def half(weight, h):
        return [weight[:, h * main : (h + 1) * main], weight[:, 2 * main + h * tail :][:, :tail]]

    def gate_up(h):
        (g, gt), (u, ut) = half(gate_weight, h), half(up_weight, h)
        return jnp.concatenate([g, u, gt, ut], axis=1)

    def down_half(h):
        return jnp.concatenate(
            [down_weight[h * main : (h + 1) * main], down_weight[2 * main + h * tail :][:tail]],
            axis=0,
        )

    first, second = gate_up(0), gate_up(1)
    gu_own, gu_far = jnp.where(low, first, second), jnp.where(low, second, first)
    first, second = down_half(0), down_half(1)
    dn_own, dn_far = jnp.where(low, first, second), jnp.where(low, second, first)

    gu_own_m = swap(gu_own, "zh")
    gu_swp = swap(gu_far, "zl")
    gu_own_y = swap(gu_own, "y")
    out_pair = jnp.concatenate([out_weight, swap(out_weight, "x")], axis=0)
    out_pair_c = swap(out_pair, "c")
    gain_pair = jnp.concatenate([norm_gain[None], swap(norm_gain[None], "x")], axis=0)
    gain_pair_c = swap(gain_pair, "c")

    attended = attention(
        queries, keys, values, query_gain, key_gain, sink_logits, ("zh", "zl", "y"), 8
    )

    gu_swp_m = swap(gu_swp, "zh")
    gu_swp_y = swap(gu_swp, "y")
    dn_swp = swap(dn_far, "zl")

    res_rows = jnp.concatenate([residual, swap(residual, "zl")], axis=0)
    res_pair = jnp.concatenate([res_rows, swap(res_rows, "x")], axis=1)
    res_pair_c = swap(res_pair, "c")

    att_rows = jnp.concatenate([attended, swap(attended, "zl")], axis=0)
    att_pair = jnp.concatenate([att_rows, swap(att_rows, "x")], axis=1)
    att_pair_c = swap(att_pair, "c")

    gu_own_my = swap(gu_own_m, "y")
    gu_swp_my = swap(gu_swp_m, "y")

    same = c == zl
    dn = jnp.concatenate(
        [jnp.where(same, dn_own, dn_swp), jnp.where(same, dn_swp, dn_own)], axis=1
    )
    dn_m = swap(dn, "zh")
    dn_y = swap(dn, "y")
    dn_my = swap(dn_m, "y")

    place = jnp.stack(
        [2 * x + c, 2 * (1 - x) + c, 2 * x + (1 - c), 2 * (1 - x) + (1 - c)]
    ).astype(jnp.int32)
    parts = [gain_pair[0], gain_pair[1], gain_pair_c[0], gain_pair_c[1]]
    gain = sum(
        jnp.where(jnp.arange(4)[:, None] == place[n], part[None], 0.0)
        for n, part in enumerate(parts)
    ).reshape(1, -1)
    normed, middle = project(
        place, att_pair, att_pair_c, out_pair, out_pair_c, res_pair, res_pair_c, gain, 256
    )

    pieces = [gu_own, gu_own_y, gu_swp, gu_swp_y, gu_own_m, gu_own_my, gu_swp_m, gu_swp_my]
    at = lambda dh, dl, dy: 4 * (zh ^ dh) + 2 * (zl ^ dl) + (y ^ dy)
    where = [(0, 0, 0), (0, 0, 1), (0, 1, 0), (0, 1, 1), (1, 0, 0), (1, 0, 1), (1, 1, 0), (1, 1, 1)]
    spots = jnp.stack([at(*w) for w in where]).astype(jnp.int32)
    hidden = hidden_units(spots, normed, pieces, main, tail, 256)

    near = x == zh

    def phase(down_near, down_far):
        mine = jnp.where(near, down_near, down_far)
        theirs = jnp.where(near, down_far, down_near)
        keep_w = jnp.concatenate([mine[:, :block], theirs[:, :block]], axis=1)
        send_w = jnp.concatenate([mine[:, block:], theirs[:, block:]], axis=1)
        sent = jnp.dot(hidden, send_w, preferred_element_type=jnp.float32).astype(jnp.bfloat16)
        got = swap(sent, "c")
        kept = jnp.dot(hidden, keep_w, preferred_element_type=jnp.float32)
        total = (kept + got.astype(jnp.float32)).astype(jnp.bfloat16)
        got = swap(total[rows:], "zl")
        total = (total[:rows].astype(jnp.float32) + got.astype(jnp.float32)).astype(jnp.bfloat16)
        got = swap(total[:, block:], "x")
        return total[:, :block].astype(jnp.float32) + got.astype(jnp.float32)

    ahead = phase(dn, dn_m)
    behind = phase(dn_y, dn_my)
    feed = jnp.where(
        y == 0,
        jnp.concatenate([ahead, behind], axis=1),
        jnp.concatenate([behind, ahead], axis=1),
    )
    return (middle[:rows].astype(jnp.float32) + 0.5 * feed).astype(jnp.bfloat16)


def solution(mesh):
    sp, tp = mesh.shape["sp"], mesh.shape["tp"]
    if (sp, tp) == (8, 4):
        fine = Mesh(mesh.devices.reshape(2, 2, 2, 2, 2), ("zh", "zl", "y", "x", "c"))
        sp_axes, tp_axes, body = ("zh", "zl", "y"), ("x", "c"), paired_device
    else:
        fine, sp_axes, tp_axes, body = mesh, "sp", "tp", None
    in_specs = (
        P(sp_axes, tp_axes),
        P(sp_axes, tp_axes),
        P(sp_axes, tp_axes),
        P(),
        P(),
        P(tp_axes),
        P(tp_axes, None),
        P(sp_axes, tp_axes),
        P(tp_axes),
        P(sp_axes, tp_axes),
        P(sp_axes, tp_axes),
        P(tp_axes, sp_axes),
    )

    def step(*args):
        run = body or functools.partial(general_device, args[8].shape[0])
        return jax.shard_map(
            run, mesh=fine, in_specs=in_specs, out_specs=P(sp_axes, tp_axes), check_vma=False
        )(*args)

    return step
```

```python
import functools

import jax
import jax.numpy as jnp
from jax import lax
from jax.experimental import pallas as pl
from jax.experimental.pallas import tpu as pltpu
from jax.sharding import Mesh
from jax.sharding import PartitionSpec as P


WINDOW = 128
EPS = 1e-06
LANES = 128
MIB = 2**20


def from_behind(block, axes, count):
    return lax.ppermute(block, axes, [(i - 1, i) for i in range(1, count)])


def norm_heads(flat, gain, heads):
    row_count = flat.shape[0]
    head_width = gain.shape[0]
    data = flat.astype(jnp.float32).reshape(row_count, heads, head_width)
    scaled = data * lax.rsqrt(jnp.mean(data * data, axis=-1, keepdims=True) + EPS) * gain
    return scaled.astype(jnp.bfloat16)


def attention(queries, keys, values, query_gain, key_gain, sink_logits, sp_axes, sp_count):
    head_width = query_gain.shape[0]
    row_count = queries.shape[0]
    q_heads = queries.shape[1] // head_width
    k_heads = keys.shape[1] // head_width
    group_size = q_heads // k_heads
    window_len = WINDOW
    block_count = row_count // window_len
    kv_width = k_heads * head_width
    query_norm = norm_heads(queries, query_gain, q_heads)
    key_norm = norm_heads(keys, key_gain, k_heads).reshape(row_count, kv_width)
    tail = jnp.concatenate(
        [key_norm[row_count - window_len :], values[row_count - window_len :]], axis=1
    )
    prev = from_behind(tail, sp_axes, sp_count)
    prev_keys, prev_values = prev[:, :kv_width], prev[:, kv_width:]
    key_all = jnp.concatenate([prev_keys, key_norm], axis=0)
    value_all = jnp.concatenate([prev_values, values], axis=0)

    def blocks(whole, own):
        return jnp.concatenate(
            [
                whole[:row_count].reshape(block_count, window_len, k_heads, head_width),
                own.reshape(block_count, window_len, k_heads, head_width),
            ],
            axis=1,
        )

    key_blocks = blocks(key_all, key_norm)
    value_blocks = blocks(value_all, values)
    query_blocks = query_norm.reshape(block_count, window_len, k_heads, group_size, head_width)
    scores = jnp.einsum(
        "nqhgd,nkhd->nhgqk", query_blocks, key_blocks, preferred_element_type=jnp.float32
    ) * head_width ** (-0.5)
    query_index = jnp.arange(window_len)[:, None]
    key_index = jnp.arange(2 * window_len)[None, :]
    offset_lag = window_len + query_index - key_index
    inband = (offset_lag >= 0) & (offset_lag < window_len)
    leading = (
        (jnp.arange(block_count)[:, None, None] > 0)
        | (key_index[None] >= window_len)
        | (lax.axis_index(sp_axes) > 0)
    )
    valid = inband[None] & leading
    scores = jnp.where(valid[:, None, None], scores, -1e30)
    sink_rows = sink_logits.reshape(k_heads, group_size)[None, :, :, None]
    row_peak = jnp.maximum(jnp.max(scores, axis=-1), sink_rows)
    exp_terms = jnp.exp(scores - row_peak[..., None])
    denom_sum = jnp.sum(exp_terms, axis=-1) + jnp.exp(sink_rows - row_peak)
    weights = (exp_terms / denom_sum[..., None]).astype(jnp.bfloat16)
    attended = jnp.einsum(
        "nhgqk,nkhd->nqhgd", weights, value_blocks, preferred_element_type=jnp.float32
    ).astype(jnp.bfloat16)
    return attended.reshape(row_count, q_heads * head_width)


def general_device(model_width, *args):
    (queries, keys, values, query_gain, key_gain, sink_logits, out_weight, residual) = args[:8]
    (norm_gain, gate_weight, up_weight, down_weight) = args[8:]
    gate_full = lax.all_gather(gate_weight, "sp", axis=0, tiled=True)
    up_full = lax.all_gather(up_weight, "sp", axis=0, tiled=True)
    down_full = lax.all_gather(down_weight, "sp", axis=1, tiled=True)
    attended = attention(
        queries, keys, values, query_gain, key_gain, sink_logits, "sp", lax.axis_size("sp")
    )
    projected = jnp.dot(attended, out_weight, preferred_element_type=jnp.float32)
    mixed = lax.psum_scatter(
        projected.astype(jnp.bfloat16), "tp", scatter_dimension=1, tiled=True
    ).astype(jnp.float32)
    middle_wide = (residual.astype(jnp.float32) + mixed).astype(jnp.bfloat16).astype(jnp.float32)
    squares = lax.psum(jnp.sum(middle_wide * middle_wide, axis=1), "tp")
    scale = lax.rsqrt(squares / model_width + EPS)[:, None]
    normed = (middle_wide * scale * norm_gain).astype(jnp.bfloat16)
    normed_all = lax.all_gather(normed, "tp", axis=1, tiled=True)
    gate_acts = jnp.dot(normed_all, gate_full, preferred_element_type=jnp.float32)
    up_acts = jnp.dot(normed_all, up_full, preferred_element_type=jnp.float32)
    hidden = (jax.nn.silu(gate_acts) * up_acts).astype(jnp.bfloat16)
    down_terms = jnp.dot(hidden, down_full, preferred_element_type=jnp.float32)
    summed_back = lax.psum_scatter(
        down_terms.astype(jnp.bfloat16), "tp", scatter_dimension=1, tiled=True
    ).astype(jnp.float32)
    return (middle_wide + 0.5 * summed_back).astype(jnp.bfloat16)


def swap(block, axis):
    return lax.ppermute(block, axis, [(0, 1), (1, 0)])


def scaled_rows(data, gain):
    wide = data.astype(jnp.float32)
    scale = lax.rsqrt(jnp.mean(wide * wide, axis=-1, keepdims=True) + EPS)
    return (wide * scale * gain).astype(jnp.bfloat16)


def attend_kernel(
    place_ref, sink_ref, q_ref, k_ref, v_ref, halo_ref, qg_ref, kg_ref, out_ref, keys, vals
):
    step = pl.program_id(0)
    width, window = k_ref.shape[0], q_ref.shape[0]
    heads = q_ref.shape[1] // width

    @pl.when(step == 0)
    def _():
        def scaled_columns(data):
            wide = data.astype(jnp.float32)
            scale = lax.rsqrt(jnp.mean(wide * wide, axis=0, keepdims=True) + EPS)
            return (wide * scale * kg_ref[...]).astype(jnp.bfloat16)

        keys[:, :window] = scaled_columns(halo_ref[:width, :])
        keys[:, window:] = scaled_columns(k_ref[...])
        vals[:, :window] = halo_ref[width:, :]
        vals[:, window:] = v_ref[...]

    span = pl.ds(pl.multiple_of(step * window, window), 2 * window)
    part = [scaled_rows(q_ref[:, h * width : (h + 1) * width], qg_ref[...]) for h in range(heads)]
    scores = jnp.dot(
        jnp.concatenate(part, axis=0), keys[:, span], preferred_element_type=jnp.float32
    ) * width ** (-0.5)
    shape = (window, 2 * window)
    column = lax.broadcasted_iota(jnp.int32, shape, 1)
    lag = window + lax.broadcasted_iota(jnp.int32, shape, 0) - column
    starts = (step > 0) | (place_ref[0] > 0)
    valid = (lag >= 0) & (lag < window) & ((column >= window) | starts)
    weights = []
    for h in range(heads):
        sink = sink_ref[h]
        score = jnp.where(valid, scores[h * window : (h + 1) * window], -1e30)
        peak = jnp.maximum(jnp.max(score, axis=-1, keepdims=True), sink)
        terms = jnp.exp(score - peak)
        total = jnp.sum(terms, axis=-1, keepdims=True) + jnp.exp(sink - peak)
        weights.append((terms / total).astype(jnp.bfloat16))
    mixed = lax.dot_general(
        jnp.concatenate(weights, axis=0),
        vals[:, span],
        (((1,), (1,)), ((), ())),
        preferred_element_type=jnp.float32,
    ).astype(jnp.bfloat16)
    out_ref[...] = jnp.concatenate(
        [mixed[h * window : (h + 1) * window] for h in range(heads)], axis=1
    )


def attend(place, sinks, queries, keys, values, halo, query_gain, key_gain):
    width, rows = keys.shape
    window = WINDOW
    full = lambda a: pl.BlockSpec(a.shape, lambda i, p, s: (0,) * a.ndim)
    row_spec = pl.BlockSpec((window, queries.shape[1]), lambda i, p, s: (i, 0))
    gains = (query_gain[None], key_gain[:, None])
    return pl.pallas_call(
        attend_kernel,
        grid_spec=pltpu.PrefetchScalarGridSpec(
            num_scalar_prefetch=2,
            grid=(rows // window,),
            in_specs=[row_spec, full(keys), full(values), full(halo), *map(full, gains)],
            out_specs=row_spec,
            scratch_shapes=[pltpu.VMEM((width, rows + window), jnp.bfloat16)] * 2,
        ),
        out_shape=jax.ShapeDtypeStruct(queries.shape, jnp.bfloat16),
        cost_estimate=pl.CostEstimate(
            flops=rows * window * width * 400, bytes_accessed=rows * 1024, transcendentals=0
        ),
        name="attend",
    )(place, sinks, queries, keys, values, halo, *gains)


def halves_kernel(main, tail, place_ref, gate_ref, up_ref, own_ref, far_ref):
    def put(ref, h):
        ref[:, :main] = gate_ref[:, h * main : (h + 1) * main]
        ref[:, main : 2 * main] = up_ref[:, h * main : (h + 1) * main]
        if tail:
            rest = [r[:, 2 * main :][:, h * tail : (h + 1) * tail] for r in (gate_ref, up_ref)]
            ref[:, 2 * main :] = jnp.concatenate(rest, axis=1)

    for low in (0, 1):

        @pl.when(place_ref[0] == low)
        def _():
            put(own_ref, low)
            put(far_ref, 1 - low)


def down_halves_kernel(main, tail, place_ref, down_ref, own_ref, far_ref):
    def put(ref, h):
        ref[:main, :] = down_ref[h * main : (h + 1) * main, :]
        if tail:
            ref[main:, :] = down_ref[2 * main + h * tail : 2 * main + (h + 1) * tail, :]

    for low in (0, 1):

        @pl.when(place_ref[0] == low)
        def _():
            put(own_ref, low)
            put(far_ref, 1 - low)


def split(kernel, place, shape, *weights):
    spec = lambda s: pl.BlockSpec(s, lambda i, p: (0, 0))
    return pl.pallas_call(
        kernel,
        grid_spec=pltpu.PrefetchScalarGridSpec(
            num_scalar_prefetch=1,
            grid=(1,),
            in_specs=[spec(w.shape) for w in weights],
            out_specs=[spec(shape)] * 2,
        ),
        out_shape=[jax.ShapeDtypeStruct(shape, jnp.bfloat16)] * 2,
        cost_estimate=pl.CostEstimate(flops=10**9, bytes_accessed=10**6, transcendentals=0),
    )(place, *weights)


def project_kernel(place_ref, *refs):
    atts, outs, ress, gains = (refs[4 * n : 4 * n + 4] for n in range(4))
    normed_ref, middle_ref, held = refs[16:]
    width = ress[0].shape[1]
    columns = [pl.ds(pl.multiple_of(place_ref[n] * width, width), width) for n in range(4)]
    squares = 0.0
    for n in range(4):
        total = sum(
            jnp.dot(a[...], o[:, columns[n]], preferred_element_type=jnp.float32)
            for a, o in zip(atts, outs)
        )
        middle = (total + ress[n][...].astype(jnp.float32)).astype(jnp.bfloat16)
        wide = middle.astype(jnp.float32)
        squares += jnp.sum(wide * wide, axis=1, keepdims=True)
        held[n] = middle
    scale = lax.rsqrt(squares / (4 * width) + EPS)
    for n in range(4):
        wide = held[n].astype(jnp.float32)
        normed_ref[:, columns[n]] = (wide * scale * gains[n][...]).astype(jnp.bfloat16)
    middle_ref[...] = held[0]


def project(place, atts, outs, ress, gains, tile):
    rows, depth = atts[0].shape
    width = outs[0].shape[1]
    part = ress[0].shape[1]
    row_spec = lambda n: pl.BlockSpec((tile, n), lambda i, p: (i, 0))
    full_spec = lambda a: pl.BlockSpec(a.shape, lambda i, p: (0, 0))
    return pl.pallas_call(
        project_kernel,
        grid_spec=pltpu.PrefetchScalarGridSpec(
            num_scalar_prefetch=1,
            grid=(rows // tile,),
            in_specs=[row_spec(depth)] * 4
            + [full_spec(o) for o in outs]
            + [row_spec(part)] * 4
            + [full_spec(g) for g in gains],
            out_specs=[row_spec(width), row_spec(part)],
            scratch_shapes=[pltpu.VMEM((4, tile, part), jnp.bfloat16)],
        ),
        out_shape=[
            jax.ShapeDtypeStruct((rows, width), jnp.bfloat16),
            jax.ShapeDtypeStruct((rows, part), jnp.bfloat16),
        ],
        compiler_params=pltpu.CompilerParams(vmem_limit_bytes=60 * MIB),
        cost_estimate=pl.CostEstimate(
            flops=8 * rows * depth * width, bytes_accessed=4 * rows * width, transcendentals=0
        ),
    )(place, *atts, *outs, *ress, *gains)


def partial_kernel(count, place_ref, x_ref, *refs):
    pieces, out_ref, whole = refs[:count], refs[count], refs[count + 1]
    depth = pieces[0].shape[0]

    @pl.when(pl.program_id(0) == 0)
    def _():
        for n, piece in enumerate(pieces):
            whole[n * depth : (n + 1) * depth, :] = piece[...]

    columns = [pl.ds(pl.multiple_of(place_ref[n] * depth, depth), depth) for n in range(count)]
    x = jnp.concatenate([x_ref[:, c] for c in columns], axis=1)
    out_ref[...] = jnp.dot(x, whole[...], preferred_element_type=jnp.float32)


def partial_acts(place, x, pieces, tile):
    rows, depth = x.shape
    count, (piece, width) = len(pieces), pieces[0].shape
    return pl.pallas_call(
        functools.partial(partial_kernel, count),
        grid_spec=pltpu.PrefetchScalarGridSpec(
            num_scalar_prefetch=1,
            grid=(rows // tile,),
            in_specs=[pl.BlockSpec((tile, depth), lambda i, p: (i, 0))]
            + [pl.BlockSpec(p.shape, lambda i, p: (0, 0)) for p in pieces],
            out_specs=pl.BlockSpec((tile, width), lambda i, p: (i, 0)),
            scratch_shapes=[pltpu.VMEM((count * piece, width), jnp.bfloat16)],
        ),
        out_shape=jax.ShapeDtypeStruct((rows, width), jnp.float32),
        compiler_params=pltpu.CompilerParams(vmem_limit_bytes=60 * MIB),
        cost_estimate=pl.CostEstimate(
            flops=2 * rows * count * piece * width, bytes_accessed=4 * rows * width,
            transcendentals=0,
        ),
    )(place, x, *pieces)


def hidden_kernel(main, tail, early, count, place_ref, near_ref, far_ref, acts_ref, *refs):
    pieces, out_ref, whole = refs[:count], refs[count], refs[count + 1]
    depth = near_ref.shape[1] // 8
    step = pl.program_id(0)
    middle = pl.num_programs(0) // 2

    @pl.when(step == 0)
    def _():
        start = 0
        for piece in pieces:
            whole[start : start + piece.shape[0], :] = piece[...]
            start += piece.shape[0]

    def gated(gate, up):
        return (gate / (1.0 + jnp.exp(-gate)) * up).astype(jnp.bfloat16)

    def product(x_ref, first):
        columns = [
            pl.ds(pl.multiple_of(place_ref[n] * depth, depth), depth) for n in range(first, 8)
        ]
        x = jnp.concatenate([x_ref[:, c] for c in columns], axis=1)
        return jnp.dot(x, whole[first * depth :, :], preferred_element_type=jnp.float32)

    def finish(acts):
        out_ref[:, :main] = gated(acts[:, :main], acts[:, main : 2 * main])
        if tail:
            rest = acts[:, 2 * main :]
            out_ref[:, main:] = gated(rest[:, :tail], rest[:, tail:])

    pl.when(step < middle)(lambda: finish(acts_ref[...] + product(near_ref, early)))
    pl.when(step >= middle)(lambda: finish(product(far_ref, 0)))


def hidden_units(place, near, far, acts, pieces, early, main, tail, tile):
    rows, depth = near.shape
    width = pieces[0].shape[1]
    tiles = rows // tile
    first = lambda i, p: (jnp.minimum(i, tiles - 1), 0)
    second = lambda i, p: (jnp.maximum(i - tiles, 0), 0)
    return pl.pallas_call(
        functools.partial(hidden_kernel, main, tail, early, len(pieces)),
        grid_spec=pltpu.PrefetchScalarGridSpec(
            num_scalar_prefetch=1,
            grid=(2 * tiles,),
            in_specs=[
                pl.BlockSpec((tile, depth), first),
                pl.BlockSpec((tile, depth), second),
                pl.BlockSpec((tile, width), first),
            ]
            + [pl.BlockSpec(p.shape, lambda i, p: (0, 0)) for p in pieces],
            out_specs=pl.BlockSpec((tile, main + tail), lambda i, p: (i, 0)),
            scratch_shapes=[pltpu.VMEM((depth, width), jnp.bfloat16)],
        ),
        out_shape=jax.ShapeDtypeStruct((2 * rows, main + tail), jnp.bfloat16),
        compiler_params=pltpu.CompilerParams(vmem_limit_bytes=40 * MIB),
        cost_estimate=pl.CostEstimate(
            flops=3 * rows * depth * width, bytes_accessed=8 * rows * width, transcendentals=0
        ),
        name="hidden_units",
    )(place, near, far, acts, *pieces)


def down_kernel(kept, flag_ref, hidden_ref, *refs):
    pieces, (*got_ref, out_ref, whole) = refs[:4], refs[4:]
    block = pieces[0].shape[1]

    @pl.when(pl.program_id(0) == 0)
    def _():
        for same in (0, 1):
            for near in (0, 1):

                @pl.when((flag_ref[0] == same) & (flag_ref[1] == near))
                def _():
                    for n, piece in enumerate(pieces):
                        if ((n % 2) != same) == kept:
                            at = block if (n // 2) == near else 0
                            whole[:, at : at + block] = piece[...]

    acts = jnp.dot(hidden_ref[...], whole[...], preferred_element_type=jnp.float32)
    if kept:
        acts += got_ref[0][...].astype(jnp.float32)
    out_ref[...] = acts.astype(jnp.bfloat16)


def down(flags, hidden, pieces, tile, got=()):
    rows, depth = hidden.shape
    block = pieces[0].shape[1]
    row_spec = lambda n: pl.BlockSpec((tile, n), lambda i, p: (i, 0))
    return pl.pallas_call(
        functools.partial(down_kernel, bool(got)),
        grid_spec=pltpu.PrefetchScalarGridSpec(
            num_scalar_prefetch=1,
            grid=(rows // tile,),
            in_specs=[row_spec(depth)]
            + [pl.BlockSpec(p.shape, lambda i, p: (0, 0)) for p in pieces]
            + [row_spec(2 * block)] * len(got),
            out_specs=row_spec(2 * block),
            scratch_shapes=[pltpu.VMEM((depth, 2 * block), jnp.bfloat16)],
        ),
        out_shape=jax.ShapeDtypeStruct((rows, 2 * block), jnp.bfloat16),
        compiler_params=pltpu.CompilerParams(vmem_limit_bytes=20 * MIB),
        cost_estimate=pl.CostEstimate(
            flops=4 * rows * depth * block, bytes_accessed=4 * rows * block, transcendentals=0
        ),
    )(flags, hidden, *pieces, *got)


def finish_kernel(flag_ref, middle_ref, ahead_ref, ahead_got, behind_ref, behind_got, out_ref):
    block = ahead_ref.shape[1]
    pairs = ((ahead_ref, ahead_got), (behind_ref, behind_got))
    for odd in (0, 1):

        @pl.when(flag_ref[0] == odd)
        def _():
            for n, (kept, got) in enumerate(pairs):
                columns = slice((n ^ odd) * block, ((n ^ odd) + 1) * block)
                feed = kept[...].astype(jnp.float32) + got[...].astype(jnp.float32)
                total = middle_ref[:, columns].astype(jnp.float32) + 0.5 * feed
                out_ref[:, columns] = total.astype(jnp.bfloat16)


def finish(flag, middle, ahead, ahead_got, behind, behind_got):
    rows, width = middle.shape
    block = ahead.shape[1]
    tile = rows // 2
    wide = pl.BlockSpec((tile, width), lambda i, p: (i, 0))
    half = pl.BlockSpec((tile, block), lambda i, p: (i, 0))
    return pl.pallas_call(
        finish_kernel,
        grid_spec=pltpu.PrefetchScalarGridSpec(
            num_scalar_prefetch=1,
            grid=(2,),
            in_specs=[wide, half, half, half, half],
            out_specs=wide,
        ),
        out_shape=jax.ShapeDtypeStruct((rows, width), jnp.bfloat16),
        cost_estimate=pl.CostEstimate(
            flops=rows * width * 8, bytes_accessed=rows * width * 8, transcendentals=0
        ),
        name="finish",
    )(flag, middle, ahead, ahead_got, behind, behind_got)


def paired_device(
    queries, keys, values, query_gain, key_gain, sink_logits, out_weight, residual, norm_gain,
    gate_weight, up_weight, down_weight,
):
    zh, zl, y, x, c = (lax.axis_index(a) for a in ("zh", "zl", "y", "x", "c"))
    rows = queries.shape[0]
    block = down_weight.shape[1]
    units = gate_weight.shape[1]
    main = units // LANES // 2 * LANES
    tail = (units - 2 * main) // 2
    one = lambda v: v.astype(jnp.int32).reshape(1)

    sp_axes = ("zh", "zl", "y")
    keys, values = keys.T, values.T
    edge = jnp.concatenate([keys[:, rows - WINDOW :], values[:, rows - WINDOW :]], axis=0)
    halo = from_behind(edge, sp_axes, lax.axis_size(sp_axes))

    gu_own, gu_far = split(
        functools.partial(halves_kernel, main, tail), one(zl),
        gate_weight.shape, gate_weight, up_weight,
    )
    gu_swp = swap(gu_far, "zl")
    gu_own_m = swap(gu_own, "zh")
    gu_own_y = swap(gu_own, "y")
    res2 = swap(residual, "zl")
    dn_own, dn_far = split(
        functools.partial(down_halves_kernel, main, tail), one(zl),
        (main + tail, block), down_weight,
    )
    attended = attend(
        one(lax.axis_index(sp_axes)), sink_logits, queries, keys, values, halo, query_gain,
        key_gain,
    )
    att2 = swap(attended, "zl")
    part = gu_swp.shape[0] // 2
    gu_swp_m = [swap(gu_swp[n * part : (n + 1) * part], "zh") for n in (0, 1)]
    gu_swp_y = swap(gu_swp, "y")
    dn_swp = swap(dn_far, "zl")
    dn_own_m = swap(dn_own, "zh")
    dn_own_y = swap(dn_own, "y")
    gu_own_my = swap(gu_own_m, "y")

    place = jnp.stack(
        [2 * x + c, 2 * (1 - x) + c, 2 * x + (1 - c), 2 * (1 - x) + (1 - c)]
    ).astype(jnp.int32)

    def over_tp(own):
        far = swap(own, "x")
        return own, far, swap(own, "c"), swap(far, "c")

    gains = over_tp(norm_gain[None])
    outs = over_tp(out_weight)
    normed, middle = project(
        place, over_tp(attended), outs, over_tp(residual), gains,
        256,
    )
    normed2, _ = project(place, over_tp(att2), outs, over_tp(res2), gains, 256)

    gu_swp_my = [swap(gu_swp_m[n], "y") for n in (0, 1)]
    dn_swp_m = swap(dn_swp, "zh")
    dn_swp_y = swap(dn_swp, "y")
    dn_own_my = swap(dn_own_m, "y")
    dn_swp_my = swap(dn_swp_m, "y")

    pieces = [gu_own, gu_own_y, gu_swp, gu_swp_y, gu_own_m, gu_own_my]
    at = lambda n: 4 * (zh ^ (n // 4)) + 2 * (zl ^ (n // 2 % 2)) + (y ^ (n % 2))
    spots = jnp.stack([at(n) for n in range(8)]).astype(jnp.int32)
    acts = partial_acts(spots[:6], normed, pieces, rows // 2)
    hidden = hidden_units(
        spots, normed, normed2, acts, [*pieces, *gu_swp_m, *gu_swp_my], 6, main, tail, rows // 2
    )

    flags = jnp.stack([c == zl, x == zh]).astype(jnp.int32)
    wide = lambda v: v.astype(jnp.float32)
    add = lambda a, b: wide(a) + wide(b)

    def reduced(pieces, rows_first):
        sent = down(flags, hidden, pieces, rows // 2)
        got = swap(sent, "c")
        total = down(flags, hidden, pieces, rows // 2, (got,))
        if rows_first:
            got = swap(total[rows:], "zl")
            total = add(total[:rows], got).astype(jnp.bfloat16)
            return total[:, :block], swap(total[:, block:], "x")
        got = swap(total[:, block:], "x")
        total = add(total[:, :block], got).astype(jnp.bfloat16)
        return total[:rows], swap(total[rows:], "zl")

    ahead = reduced((dn_own, dn_swp, dn_own_m, dn_swp_m), True)
    behind = reduced((dn_own_y, dn_swp_y, dn_own_my, dn_swp_my), False)
    return finish(one(y), middle, *ahead, *behind)


def solution(mesh):
    sp, tp = mesh.shape["sp"], mesh.shape["tp"]

    def spread(fine, sp_axes, tp_axes, body):
        both = P(sp_axes, tp_axes)
        heads, rows = P(tp_axes), P(tp_axes, None)
        in_specs = (both, both, both, P(), P(), heads, rows, both, heads, both, both)
        return jax.shard_map(
            body,
            mesh=fine,
            in_specs=(*in_specs, P(tp_axes, sp_axes)),
            out_specs=both,
            check_vma=False,
        )

    def step(*args):
        if (sp, tp) == (8, 4) and args[1].shape[1] == tp * args[3].shape[0]:
            fine = Mesh(mesh.devices.reshape(2, 2, 2, 2, 2), ("zh", "zl", "y", "x", "c"))
            return spread(fine, ("zh", "zl", "y"), ("x", "c"), paired_device)(*args)
        body = functools.partial(general_device, args[8].shape[0])
        return spread(mesh, "sp", "tp", body)(*args)

    return step
```

```python
import functools

import jax
import jax.numpy as jnp
from jax import lax
from jax.experimental import pallas as pl
from jax.experimental.pallas import tpu as pltpu
from jax.sharding import Mesh
from jax.sharding import PartitionSpec as P


WINDOW = 128
EPS = 1e-06
LANES = 128
MIB = 2**20
PROJECT_MIB, PARTIAL_MIB, HIDDEN_MIB, NEAR_MIB, DOWN_MIB = 60, 60, 56, 56, 24


def from_behind(block, axes, count):
    return lax.ppermute(block, axes, [(i - 1, i) for i in range(1, count)])


def norm_heads(flat, gain, heads):
    row_count = flat.shape[0]
    head_width = gain.shape[0]
    data = flat.astype(jnp.float32).reshape(row_count, heads, head_width)
    scaled = data * lax.rsqrt(jnp.mean(data * data, axis=-1, keepdims=True) + EPS) * gain
    return scaled.astype(jnp.bfloat16)


def attention(queries, keys, values, query_gain, key_gain, sink_logits, sp_axes, sp_count):
    head_width = query_gain.shape[0]
    row_count = queries.shape[0]
    q_heads = queries.shape[1] // head_width
    k_heads = keys.shape[1] // head_width
    group_size = q_heads // k_heads
    window_len = WINDOW
    block_count = row_count // window_len
    kv_width = k_heads * head_width
    query_norm = norm_heads(queries, query_gain, q_heads)
    key_norm = norm_heads(keys, key_gain, k_heads).reshape(row_count, kv_width)
    tail = jnp.concatenate(
        [key_norm[row_count - window_len :], values[row_count - window_len :]], axis=1
    )
    prev = from_behind(tail, sp_axes, sp_count)
    prev_keys, prev_values = prev[:, :kv_width], prev[:, kv_width:]
    key_all = jnp.concatenate([prev_keys, key_norm], axis=0)
    value_all = jnp.concatenate([prev_values, values], axis=0)

    def blocks(whole, own):
        return jnp.concatenate(
            [
                whole[:row_count].reshape(block_count, window_len, k_heads, head_width),
                own.reshape(block_count, window_len, k_heads, head_width),
            ],
            axis=1,
        )

    key_blocks = blocks(key_all, key_norm)
    value_blocks = blocks(value_all, values)
    query_blocks = query_norm.reshape(block_count, window_len, k_heads, group_size, head_width)
    scores = jnp.einsum(
        "nqhgd,nkhd->nhgqk", query_blocks, key_blocks, preferred_element_type=jnp.float32
    ) * head_width ** (-0.5)
    query_index = jnp.arange(window_len)[:, None]
    key_index = jnp.arange(2 * window_len)[None, :]
    offset_lag = window_len + query_index - key_index
    inband = (offset_lag >= 0) & (offset_lag < window_len)
    leading = (
        (jnp.arange(block_count)[:, None, None] > 0)
        | (key_index[None] >= window_len)
        | (lax.axis_index(sp_axes) > 0)
    )
    valid = inband[None] & leading
    scores = jnp.where(valid[:, None, None], scores, -1e30)
    sink_rows = sink_logits.reshape(k_heads, group_size)[None, :, :, None]
    row_peak = jnp.maximum(jnp.max(scores, axis=-1), sink_rows)
    exp_terms = jnp.exp(scores - row_peak[..., None])
    denom_sum = jnp.sum(exp_terms, axis=-1) + jnp.exp(sink_rows - row_peak)
    weights = (exp_terms / denom_sum[..., None]).astype(jnp.bfloat16)
    attended = jnp.einsum(
        "nhgqk,nkhd->nqhgd", weights, value_blocks, preferred_element_type=jnp.float32
    ).astype(jnp.bfloat16)
    return attended.reshape(row_count, q_heads * head_width)


def general_device(model_width, *args):
    (queries, keys, values, query_gain, key_gain, sink_logits, out_weight, residual) = args[:8]
    (norm_gain, gate_weight, up_weight, down_weight) = args[8:]
    gate_full = lax.all_gather(gate_weight, "sp", axis=0, tiled=True)
    up_full = lax.all_gather(up_weight, "sp", axis=0, tiled=True)
    down_full = lax.all_gather(down_weight, "sp", axis=1, tiled=True)
    attended = attention(
        queries, keys, values, query_gain, key_gain, sink_logits, "sp", lax.axis_size("sp")
    )
    projected = jnp.dot(attended, out_weight, preferred_element_type=jnp.float32)
    mixed = lax.psum_scatter(
        projected.astype(jnp.bfloat16), "tp", scatter_dimension=1, tiled=True
    ).astype(jnp.float32)
    middle_wide = (residual.astype(jnp.float32) + mixed).astype(jnp.bfloat16).astype(jnp.float32)
    squares = lax.psum(jnp.sum(middle_wide * middle_wide, axis=1), "tp")
    scale = lax.rsqrt(squares / model_width + EPS)[:, None]
    normed = (middle_wide * scale * norm_gain).astype(jnp.bfloat16)
    normed_all = lax.all_gather(normed, "tp", axis=1, tiled=True)
    gate_acts = jnp.dot(normed_all, gate_full, preferred_element_type=jnp.float32)
    up_acts = jnp.dot(normed_all, up_full, preferred_element_type=jnp.float32)
    hidden = (jax.nn.silu(gate_acts) * up_acts).astype(jnp.bfloat16)
    down_terms = jnp.dot(hidden, down_full, preferred_element_type=jnp.float32)
    summed_back = lax.psum_scatter(
        down_terms.astype(jnp.bfloat16), "tp", scatter_dimension=1, tiled=True
    ).astype(jnp.float32)
    return (middle_wide + 0.5 * summed_back).astype(jnp.bfloat16)


def swap(block, axis):
    return lax.ppermute(block, axis, [(0, 1), (1, 0)])


def scaled_rows(data, gain):
    wide = data.astype(jnp.float32)
    scale = lax.rsqrt(jnp.mean(wide * wide, axis=-1, keepdims=True) + EPS)
    return (wide * scale * gain).astype(jnp.bfloat16)


def attend_kernel(
    place_ref, sink_ref, q_ref, k_ref, v_ref, halo_ref, qg_ref, kg_ref, out_ref, keys, vals
):
    step = pl.program_id(0)
    width, window = k_ref.shape[0], q_ref.shape[0]
    heads = q_ref.shape[1] // width

    @pl.when(step == 0)
    def _():
        def scaled_columns(data):
            wide = data.astype(jnp.float32)
            scale = lax.rsqrt(jnp.mean(wide * wide, axis=0, keepdims=True) + EPS)
            return (wide * scale * kg_ref[...]).astype(jnp.bfloat16)

        keys[:, :window] = scaled_columns(halo_ref[:width, :])
        keys[:, window:] = scaled_columns(k_ref[...])
        vals[:, :window] = halo_ref[width:, :]
        vals[:, window:] = v_ref[...]

    span = pl.ds(pl.multiple_of(step * window, window), 2 * window)
    part = [scaled_rows(q_ref[:, h * width : (h + 1) * width], qg_ref[...]) for h in range(heads)]
    scores = jnp.dot(
        jnp.concatenate(part, axis=0), keys[:, span], preferred_element_type=jnp.float32
    ) * width ** (-0.5)
    shape = (window, 2 * window)
    column = lax.broadcasted_iota(jnp.int32, shape, 1)
    lag = window + lax.broadcasted_iota(jnp.int32, shape, 0) - column
    starts = (step > 0) | (place_ref[0] > 0)
    valid = (lag >= 0) & (lag < window) & ((column >= window) | starts)
    weights = []
    for h in range(heads):
        sink = sink_ref[h]
        score = jnp.where(valid, scores[h * window : (h + 1) * window], -1e30)
        peak = jnp.maximum(jnp.max(score, axis=-1, keepdims=True), sink)
        terms = jnp.exp(score - peak)
        total = jnp.sum(terms, axis=-1, keepdims=True) + jnp.exp(sink - peak)
        weights.append((terms / total).astype(jnp.bfloat16))
    mixed = lax.dot_general(
        jnp.concatenate(weights, axis=0),
        vals[:, span],
        (((1,), (1,)), ((), ())),
        preferred_element_type=jnp.float32,
    ).astype(jnp.bfloat16)
    out_ref[...] = jnp.concatenate(
        [mixed[h * window : (h + 1) * window] for h in range(heads)], axis=1
    )


def attend(place, sinks, queries, keys, values, halo, query_gain, key_gain):
    width, rows = keys.shape
    window = WINDOW
    full = lambda a: pl.BlockSpec(a.shape, lambda i, p, s: (0,) * a.ndim)
    row_spec = pl.BlockSpec((window, queries.shape[1]), lambda i, p, s: (i, 0))
    gains = (query_gain[None], key_gain[:, None])
    return pl.pallas_call(
        attend_kernel,
        grid_spec=pltpu.PrefetchScalarGridSpec(
            num_scalar_prefetch=2,
            grid=(rows // window,),
            in_specs=[row_spec, full(keys), full(values), full(halo), *map(full, gains)],
            out_specs=row_spec,
            scratch_shapes=[pltpu.VMEM((width, rows + window), jnp.bfloat16)] * 2,
        ),
        out_shape=jax.ShapeDtypeStruct(queries.shape, jnp.bfloat16),
        cost_estimate=pl.CostEstimate(
            flops=rows * window * width * 400, bytes_accessed=rows * 1024, transcendentals=0
        ),
        name="attend",
    )(place, sinks, queries, keys, values, halo, *gains)


def halves_kernel(main, tail, place_ref, gate_ref, up_ref, *outs):
    def put(refs, h):
        start = 0
        for ref in refs:
            rows = slice(start, start + ref.shape[0])
            start += ref.shape[0]
            ref[:, :main] = gate_ref[rows, h * main : (h + 1) * main]
            ref[:, main : 2 * main] = up_ref[rows, h * main : (h + 1) * main]
            if tail:
                rest = [r[rows, 2 * main :][:, h * tail :][:, :tail] for r in (gate_ref, up_ref)]
                ref[:, 2 * main :] = jnp.concatenate(rest, axis=1)

    for low in (0, 1):

        @pl.when(place_ref[0] == low)
        def _():
            put(outs[:1], low)
            put(outs[1:], 1 - low)


def down_halves_kernel(main, tail, place_ref, down_ref, own_ref, far_ref):
    def put(ref, h):
        ref[:main, :] = down_ref[h * main : (h + 1) * main, :]
        if tail:
            ref[main:, :] = down_ref[2 * main + h * tail : 2 * main + (h + 1) * tail, :]

    for low in (0, 1):

        @pl.when(place_ref[0] == low)
        def _():
            put(own_ref, low)
            put(far_ref, 1 - low)


def split(kernel, place, shapes, *weights):
    spec = lambda s: pl.BlockSpec(s, lambda i, p: (0, 0))
    return pl.pallas_call(
        kernel,
        grid_spec=pltpu.PrefetchScalarGridSpec(
            num_scalar_prefetch=1,
            grid=(1,),
            in_specs=[spec(w.shape) for w in weights],
            out_specs=[spec(s) for s in shapes],
        ),
        out_shape=[jax.ShapeDtypeStruct(s, jnp.bfloat16) for s in shapes],
        cost_estimate=pl.CostEstimate(flops=10**9, bytes_accessed=10**6, transcendentals=0),
    )(place, *weights)


def normed_rows(columns, atts, outs, ress, gains, held, normed_ref):
    width = ress[0].shape[1]
    squares = 0.0
    for n in range(4):
        total = sum(
            jnp.dot(a[...], o[:, columns[n]], preferred_element_type=jnp.float32)
            for a, o in zip(atts, outs)
        )
        middle = (total + ress[n][...].astype(jnp.float32)).astype(jnp.bfloat16)
        wide = middle.astype(jnp.float32)
        squares += jnp.sum(wide * wide, axis=1, keepdims=True)
        held[n] = middle
    scale = lax.rsqrt(squares / (4 * width) + EPS)
    for n in range(4):
        wide = held[n].astype(jnp.float32)
        normed_ref[:, columns[n]] = (wide * scale * gains[n][...]).astype(jnp.bfloat16)


def spans(place_ref, first, count, width):
    return [
        pl.ds(pl.multiple_of(place_ref[first + n] * width, width), width) for n in range(count)
    ]


def project_kernel(place_ref, *refs):
    atts, outs, ress, gains = (refs[4 * n : 4 * n + 4] for n in range(4))
    normed_ref, middle_ref, held = refs[16:]
    columns = spans(place_ref, 0, 4, ress[0].shape[1])
    normed_rows(columns, atts, outs, ress, gains, held, normed_ref)
    middle_ref[...] = held[0]


def project(place, atts, outs, ress, gains, tile):
    rows, depth = atts[0].shape
    width = outs[0].shape[1]
    part = ress[0].shape[1]
    row_spec = lambda n: pl.BlockSpec((tile, n), lambda i, p: (i, 0))
    full_spec = lambda a: pl.BlockSpec(a.shape, lambda i, p: (0, 0))
    return pl.pallas_call(
        project_kernel,
        grid_spec=pltpu.PrefetchScalarGridSpec(
            num_scalar_prefetch=1,
            grid=(rows // tile,),
            in_specs=[row_spec(depth)] * 4
            + [full_spec(o) for o in outs]
            + [row_spec(part)] * 4
            + [full_spec(g) for g in gains],
            out_specs=[row_spec(width), row_spec(part)],
            scratch_shapes=[pltpu.VMEM((4, tile, part), jnp.bfloat16)],
        ),
        out_shape=[
            jax.ShapeDtypeStruct((rows, width), jnp.bfloat16),
            jax.ShapeDtypeStruct((rows, part), jnp.bfloat16),
        ],
        compiler_params=pltpu.CompilerParams(vmem_limit_bytes=PROJECT_MIB * MIB),
        cost_estimate=pl.CostEstimate(
            flops=8 * rows * depth * width, bytes_accessed=4 * rows * width, transcendentals=0
        ),
    )(place, *atts, *outs, *ress, *gains)


def stack_pieces(pieces, whole):
    start = 0
    for piece in pieces:
        whole[start : start + piece.shape[0], :] = piece[...]
        start += piece.shape[0]


def put_hidden(main, tail, acts, out_ref):
    def gated(gate, up):
        return (gate / (1.0 + jnp.exp(-gate)) * up).astype(jnp.bfloat16)

    out_ref[:, :main] = gated(acts[:, :main], acts[:, main : 2 * main])
    if tail:
        rest = acts[:, 2 * main :]
        out_ref[:, main:] = gated(rest[:, :tail], rest[:, tail:])


def product(columns, x_ref, whole):
    x = jnp.concatenate([x_ref[:, c] for c in columns], axis=1)
    return jnp.dot(x, whole[...], preferred_element_type=jnp.float32)


def far_kernel(main, tail, count, place_ref, *refs):
    atts, outs, ress, gains = (refs[4 * n : 4 * n + 4] for n in range(4))
    pieces, (out_ref, whole, held, x_ref) = refs[16 : 16 + count], refs[16 + count :]
    pl.when(pl.program_id(0) == 0)(lambda: stack_pieces(pieces, whole))
    columns = spans(place_ref, 0, 4, ress[0].shape[1])
    normed_rows(columns, atts, outs, ress, gains, held, x_ref)
    acts = product(spans(place_ref, 4, 8, x_ref.shape[1] // 8), x_ref, whole)
    put_hidden(main, tail, acts, out_ref)


def far_hidden(place, atts, outs, ress, gains, pieces, main, tail, tile):
    rows, part = ress[0].shape
    depth = sum(p.shape[0] for p in pieces)
    width = pieces[0].shape[1]
    tiles = rows // tile
    row_spec = lambda a: pl.BlockSpec((tile, a.shape[1]), lambda i, p: (i, 0))
    full = lambda a: pl.BlockSpec(a.shape, lambda i, p: (0, 0), pipeline_mode=pl.Buffered(1))
    operands = [*atts, *outs, *ress, *gains, *pieces]
    specs = [*map(row_spec, atts), *map(full, outs), *map(row_spec, ress)]
    return pl.pallas_call(
        functools.partial(far_kernel, main, tail, len(pieces)),
        grid_spec=pltpu.PrefetchScalarGridSpec(
            num_scalar_prefetch=1,
            grid=(tiles,),
            in_specs=[*specs, *map(full, [*gains, *pieces])],
            out_specs=pl.BlockSpec((tile, main + tail), lambda i, p: (i, 0)),
            scratch_shapes=[
                pltpu.VMEM((depth, width), jnp.bfloat16),
                pltpu.VMEM((4, tile, part), jnp.bfloat16),
                pltpu.VMEM((tile, depth), jnp.bfloat16),
            ],
        ),
        out_shape=jax.ShapeDtypeStruct((rows, main + tail), jnp.bfloat16),
        compiler_params=pltpu.CompilerParams(vmem_limit_bytes=HIDDEN_MIB * MIB),
        cost_estimate=pl.CostEstimate(
            flops=4 * rows * depth * width, bytes_accessed=8 * rows * width, transcendentals=0
        ),
        name="far_hidden",
    )(place, *operands)


def partial_kernel(count, place_ref, x_ref, *refs):
    pieces, out_ref, whole = refs[:count], refs[count], refs[count + 1]
    pl.when(pl.program_id(0) == 0)(lambda: stack_pieces(pieces, whole))
    depth = x_ref.shape[1] // 8
    columns = spans(place_ref, 4, whole.shape[0] // depth, depth)
    out_ref[...] = product(columns, x_ref, whole)


def near_kernel(main, tail, count, place_ref, x_ref, acts_ref, *refs):
    pieces, (out_ref, whole) = refs[:count], refs[count:]
    pl.when(pl.program_id(0) == 0)(lambda: stack_pieces(pieces, whole))
    depth = x_ref.shape[1] // 8
    blocks = whole.shape[0] // depth
    columns = spans(place_ref, 12 - blocks, blocks, depth)
    put_hidden(main, tail, acts_ref[...] + product(columns, x_ref, whole), out_ref)


def near_step(kernel, place, x, more, pieces, out_shape, limit, tile):
    rows, _ = x.shape
    total = sum(p.shape[0] for p in pieces)
    row_spec = lambda a: pl.BlockSpec((tile, a.shape[1]), lambda i, p: (i, 0))
    full = lambda a: pl.BlockSpec(a.shape, lambda i, p: (0, 0), pipeline_mode=pl.Buffered(1))
    return pl.pallas_call(
        kernel,
        grid_spec=pltpu.PrefetchScalarGridSpec(
            num_scalar_prefetch=1,
            grid=(rows // tile,),
            in_specs=[row_spec(x), *map(row_spec, more), *map(full, pieces)],
            out_specs=row_spec(out_shape),
            scratch_shapes=[pltpu.VMEM((total, pieces[0].shape[1]), jnp.bfloat16)],
        ),
        out_shape=out_shape,
        compiler_params=pltpu.CompilerParams(vmem_limit_bytes=limit * MIB),
        cost_estimate=pl.CostEstimate(
            flops=3000 * rows * total, bytes_accessed=4000 * rows, transcendentals=0
        ),
    )(place, x, *more, *pieces)


def down_kernel(kept, flag_ref, near_ref, far_ref, *refs):
    pieces, (*got_ref, out_ref, whole) = refs[:4], refs[4:]
    block = pieces[0].shape[1]

    @pl.when(pl.program_id(0) == 0)
    def _():
        for same in (0, 1):
            for near in (0, 1):

                @pl.when((flag_ref[0] == same) & (flag_ref[1] == near))
                def _():
                    for n, piece in enumerate(pieces):
                        if ((n % 2) != same) == kept:
                            at = block if (n // 2) == near else 0
                            whole[:, at : at + block] = piece[...]

    def put(hidden_ref):
        acts = jnp.dot(hidden_ref[...], whole[...], preferred_element_type=jnp.float32)
        if kept:
            acts += got_ref[0][...].astype(jnp.float32)
        out_ref[...] = acts.astype(jnp.bfloat16)

    pl.when(pl.program_id(0) == 0)(lambda: put(near_ref))
    pl.when(pl.program_id(0) == 1)(lambda: put(far_ref))


def down(flags, near, far, pieces, got=()):
    rows, depth = near.shape
    block = pieces[0].shape[1]
    row_spec = pl.BlockSpec((rows, 2 * block), lambda i, p: (i, 0))
    full = lambda a: pl.BlockSpec(a.shape, lambda i, p: (0, 0))
    return pl.pallas_call(
        functools.partial(down_kernel, bool(got)),
        grid_spec=pltpu.PrefetchScalarGridSpec(
            num_scalar_prefetch=1,
            grid=(2,),
            in_specs=[full(near), full(far), *map(full, pieces)] + [row_spec] * len(got),
            out_specs=row_spec,
            scratch_shapes=[pltpu.VMEM((depth, 2 * block), jnp.bfloat16)],
        ),
        out_shape=jax.ShapeDtypeStruct((2 * rows, 2 * block), jnp.bfloat16),
        compiler_params=pltpu.CompilerParams(vmem_limit_bytes=DOWN_MIB * MIB),
        cost_estimate=pl.CostEstimate(
            flops=8 * rows * depth * block, bytes_accessed=8 * rows * block, transcendentals=0
        ),
    )(flags, near, far, *pieces, *got)


def finish_kernel(flag_ref, middle_ref, ahead_ref, ahead_got, behind_ref, behind_got, out_ref):
    block = ahead_ref.shape[1]
    pairs = ((ahead_ref, ahead_got), (behind_ref, behind_got))
    for odd in (0, 1):

        @pl.when(flag_ref[0] == odd)
        def _():
            for n, (kept, got) in enumerate(pairs):
                columns = slice((n ^ odd) * block, ((n ^ odd) + 1) * block)
                feed = kept[...].astype(jnp.float32) + got[...].astype(jnp.float32)
                total = middle_ref[:, columns].astype(jnp.float32) + 0.5 * feed
                out_ref[:, columns] = total.astype(jnp.bfloat16)


def finish(flag, middle, ahead, ahead_got, behind, behind_got):
    rows, width = middle.shape
    block = ahead.shape[1]
    tile = rows // 2
    wide = pl.BlockSpec((tile, width), lambda i, p: (i, 0))
    half = pl.BlockSpec((tile, block), lambda i, p: (i, 0))
    return pl.pallas_call(
        finish_kernel,
        grid_spec=pltpu.PrefetchScalarGridSpec(
            num_scalar_prefetch=1,
            grid=(2,),
            in_specs=[wide, half, half, half, half],
            out_specs=wide,
        ),
        out_shape=jax.ShapeDtypeStruct((rows, width), jnp.bfloat16),
        cost_estimate=pl.CostEstimate(
            flops=rows * width * 8, bytes_accessed=rows * width * 8, transcendentals=0
        ),
        name="finish",
    )(flag, middle, ahead, ahead_got, behind, behind_got)


def paired_device(
    queries, keys, values, query_gain, key_gain, sink_logits, out_weight, residual, norm_gain,
    gate_weight, up_weight, down_weight,
):
    zh, zl, y, x, c = (lax.axis_index(a) for a in ("zh", "zl", "y", "x", "c"))
    rows = queries.shape[0]
    block = down_weight.shape[1]
    units = gate_weight.shape[1]
    main = units // LANES // 2 * LANES
    tail = (units - 2 * main) // 2
    one = lambda v: v.astype(jnp.int32).reshape(1)

    sp_axes = ("zh", "zl", "y")
    keys, values = keys.T, values.T
    edge = jnp.concatenate([keys[:, rows - WINDOW :], values[:, rows - WINDOW :]], axis=0)
    halo = from_behind(edge, sp_axes, lax.axis_size(sp_axes))

    depth = gate_weight.shape[0]
    gu_own, *gu_far = split(
        functools.partial(halves_kernel, main, tail), one(zl),
        [(depth, units), (depth // 2, units), (depth // 2, units)], gate_weight, up_weight,
    )
    pair = lambda parts, axis: [swap(parts[n], axis) for n in (0, 1)]
    gu_swp = pair(gu_far, "zl")
    gu_own_m = swap(gu_own, "zh")
    gu_own_y = swap(gu_own, "y")
    res2 = swap(residual, "zl")
    dn_own, dn_far = split(
        functools.partial(down_halves_kernel, main, tail), one(zl),
        [(main + tail, block)] * 2, down_weight,
    )
    attended = attend(
        one(lax.axis_index(sp_axes)), sink_logits, queries, keys, values, halo, query_gain,
        key_gain,
    )
    att2 = swap(attended, "zl")
    gu_swp_m = pair(gu_swp, "zh")
    gu_swp_y = pair(gu_swp, "y")
    dn_swp = swap(dn_far, "zl")
    dn_own_m = swap(dn_own, "zh")
    dn_own_y = swap(dn_own, "y")
    gu_own_my = swap(gu_own_m, "y")

    place = jnp.stack(
        [2 * x + c, 2 * (1 - x) + c, 2 * x + (1 - c), 2 * (1 - x) + (1 - c)]
    ).astype(jnp.int32)

    def over_tp(own):
        far = swap(own, "x")
        return own, far, swap(own, "c"), swap(far, "c")

    gains = over_tp(norm_gain[None])
    outs = over_tp(out_weight)
    normed, middle = project(
        place, over_tp(attended), outs, over_tp(residual), gains,
        rows // 2,
    )
    att2s, res2s = over_tp(att2), over_tp(res2)

    gu_swp_my = pair(gu_swp_m, "y")
    dn_swp_m = swap(dn_swp, "zh")
    dn_swp_y = swap(dn_swp, "y")
    dn_own_my = swap(dn_own_m, "y")
    dn_swp_my = swap(dn_swp_m, "y")

    pieces = [gu_own, gu_own_y, *gu_swp, *gu_swp_y, gu_own_m, gu_own_my]
    at = lambda n: 4 * (zh ^ (n // 4)) + 2 * (zl ^ (n // 2 % 2)) + (y ^ (n % 2))
    spots = jnp.stack([at(n) for n in range(8)]).astype(jnp.int32)
    last = [*gu_swp_m, *gu_swp_my]
    where = jnp.concatenate([place, spots])
    acts = near_step(
        functools.partial(partial_kernel, len(pieces)), where, normed, (), pieces,
        jax.ShapeDtypeStruct((rows, units), jnp.float32), PARTIAL_MIB, rows // 2,
    )
    near = near_step(
        functools.partial(near_kernel, main, tail, len(last)), where, normed,
        (acts,), last, jax.ShapeDtypeStruct((rows, main + tail), jnp.bfloat16), NEAR_MIB,
        rows // 2,
    )
    pieces += last
    far = far_hidden(where, att2s, outs, res2s, gains, pieces, main, tail, rows // 2)

    flags = jnp.stack([c == zl, x == zh]).astype(jnp.int32)
    wide = lambda v: v.astype(jnp.float32)
    add = lambda a, b: wide(a) + wide(b)

    def reduced(pieces, rows_first):
        sent = down(flags, near, far, pieces)
        got = swap(sent, "c")
        total = down(flags, near, far, pieces, (got,))
        if rows_first:
            got = swap(total[rows:], "zl")
            total = add(total[:rows], got).astype(jnp.bfloat16)
            return total[:, :block], swap(total[:, block:], "x")
        got = swap(total[:, block:], "x")
        total = add(total[:, :block], got).astype(jnp.bfloat16)
        return total[:rows], swap(total[rows:], "zl")

    ahead = reduced((dn_own, dn_swp, dn_own_m, dn_swp_m), True)
    behind = reduced((dn_own_y, dn_swp_y, dn_own_my, dn_swp_my), False)
    return finish(one(y), middle, *ahead, *behind)


def solution(mesh):
    sp, tp = mesh.shape["sp"], mesh.shape["tp"]

    def spread(fine, sp_axes, tp_axes, body):
        both = P(sp_axes, tp_axes)
        heads, rows = P(tp_axes), P(tp_axes, None)
        in_specs = (both, both, both, P(), P(), heads, rows, both, heads, both, both)
        return jax.shard_map(
            body,
            mesh=fine,
            in_specs=(*in_specs, P(tp_axes, sp_axes)),
            out_specs=both,
            check_vma=False,
        )

    def step(*args):
        if (sp, tp) == (8, 4) and args[1].shape[1] == tp * args[3].shape[0]:
            fine = Mesh(mesh.devices.reshape(2, 2, 2, 2, 2), ("zh", "zl", "y", "x", "c"))
            return spread(fine, ("zh", "zl", "y"), ("x", "c"), paired_device)(*args)
        body = functools.partial(general_device, args[8].shape[0])
        return spread(mesh, "sp", "tp", body)(*args)

    return step
```

```python
import functools

import jax
import jax.numpy as jnp
from jax import lax
from jax.experimental import pallas as pl
from jax.experimental.pallas import tpu as pltpu
from jax.sharding import Mesh
from jax.sharding import PartitionSpec as P


WINDOW = 128
EPS = 1e-06
LANES = 128
MIB = 2**20
PROJECT_MIB, PARTIAL_MIB, HIDDEN_MIB, NEAR_MIB, DOWN_MIB = 60, 60, 60, 50, 24


def from_behind(block, axes, count):
    return lax.ppermute(block, axes, [(i - 1, i) for i in range(1, count)])


def norm_heads(flat, gain, heads):
    row_count = flat.shape[0]
    head_width = gain.shape[0]
    data = flat.astype(jnp.float32).reshape(row_count, heads, head_width)
    scaled = data * lax.rsqrt(jnp.mean(data * data, axis=-1, keepdims=True) + EPS) * gain
    return scaled.astype(jnp.bfloat16)


def attention(queries, keys, values, query_gain, key_gain, sink_logits, sp_axes, sp_count):
    head_width = query_gain.shape[0]
    row_count = queries.shape[0]
    q_heads = queries.shape[1] // head_width
    k_heads = keys.shape[1] // head_width
    group_size = q_heads // k_heads
    window_len = WINDOW
    block_count = row_count // window_len
    kv_width = k_heads * head_width
    query_norm = norm_heads(queries, query_gain, q_heads)
    key_norm = norm_heads(keys, key_gain, k_heads).reshape(row_count, kv_width)
    tail = jnp.concatenate(
        [key_norm[row_count - window_len :], values[row_count - window_len :]], axis=1
    )
    prev = from_behind(tail, sp_axes, sp_count)
    prev_keys, prev_values = prev[:, :kv_width], prev[:, kv_width:]
    key_all = jnp.concatenate([prev_keys, key_norm], axis=0)
    value_all = jnp.concatenate([prev_values, values], axis=0)

    def blocks(whole, own):
        return jnp.concatenate(
            [
                whole[:row_count].reshape(block_count, window_len, k_heads, head_width),
                own.reshape(block_count, window_len, k_heads, head_width),
            ],
            axis=1,
        )

    key_blocks = blocks(key_all, key_norm)
    value_blocks = blocks(value_all, values)
    query_blocks = query_norm.reshape(block_count, window_len, k_heads, group_size, head_width)
    scores = jnp.einsum(
        "nqhgd,nkhd->nhgqk", query_blocks, key_blocks, preferred_element_type=jnp.float32
    ) * head_width ** (-0.5)
    query_index = jnp.arange(window_len)[:, None]
    key_index = jnp.arange(2 * window_len)[None, :]
    offset_lag = window_len + query_index - key_index
    inband = (offset_lag >= 0) & (offset_lag < window_len)
    leading = (
        (jnp.arange(block_count)[:, None, None] > 0)
        | (key_index[None] >= window_len)
        | (lax.axis_index(sp_axes) > 0)
    )
    valid = inband[None] & leading
    scores = jnp.where(valid[:, None, None], scores, -1e30)
    sink_rows = sink_logits.reshape(k_heads, group_size)[None, :, :, None]
    row_peak = jnp.maximum(jnp.max(scores, axis=-1), sink_rows)
    exp_terms = jnp.exp(scores - row_peak[..., None])
    denom_sum = jnp.sum(exp_terms, axis=-1) + jnp.exp(sink_rows - row_peak)
    weights = (exp_terms / denom_sum[..., None]).astype(jnp.bfloat16)
    attended = jnp.einsum(
        "nhgqk,nkhd->nqhgd", weights, value_blocks, preferred_element_type=jnp.float32
    ).astype(jnp.bfloat16)
    return attended.reshape(row_count, q_heads * head_width)


def general_device(model_width, *args):
    (queries, keys, values, query_gain, key_gain, sink_logits, out_weight, residual) = args[:8]
    (norm_gain, gate_weight, up_weight, down_weight) = args[8:]
    gate_full = lax.all_gather(gate_weight, "sp", axis=0, tiled=True)
    up_full = lax.all_gather(up_weight, "sp", axis=0, tiled=True)
    down_full = lax.all_gather(down_weight, "sp", axis=1, tiled=True)
    attended = attention(
        queries, keys, values, query_gain, key_gain, sink_logits, "sp", lax.axis_size("sp")
    )
    projected = jnp.dot(attended, out_weight, preferred_element_type=jnp.float32)
    mixed = lax.psum_scatter(
        projected.astype(jnp.bfloat16), "tp", scatter_dimension=1, tiled=True
    ).astype(jnp.float32)
    middle_wide = (residual.astype(jnp.float32) + mixed).astype(jnp.bfloat16).astype(jnp.float32)
    squares = lax.psum(jnp.sum(middle_wide * middle_wide, axis=1), "tp")
    scale = lax.rsqrt(squares / model_width + EPS)[:, None]
    normed = (middle_wide * scale * norm_gain).astype(jnp.bfloat16)
    normed_all = lax.all_gather(normed, "tp", axis=1, tiled=True)
    gate_acts = jnp.dot(normed_all, gate_full, preferred_element_type=jnp.float32)
    up_acts = jnp.dot(normed_all, up_full, preferred_element_type=jnp.float32)
    hidden = (jax.nn.silu(gate_acts) * up_acts).astype(jnp.bfloat16)
    down_terms = jnp.dot(hidden, down_full, preferred_element_type=jnp.float32)
    summed_back = lax.psum_scatter(
        down_terms.astype(jnp.bfloat16), "tp", scatter_dimension=1, tiled=True
    ).astype(jnp.float32)
    return (middle_wide + 0.5 * summed_back).astype(jnp.bfloat16)


def swap(block, axis):
    return lax.ppermute(block, axis, [(0, 1), (1, 0)])


def scaled_rows(data, gain):
    wide = data.astype(jnp.float32)
    scale = lax.rsqrt(jnp.mean(wide * wide, axis=-1, keepdims=True) + EPS)
    return (wide * scale * gain).astype(jnp.bfloat16)


def attend_kernel(
    place_ref, sink_ref, q_ref, k_ref, v_ref, halo_ref, qg_ref, kg_ref, out_ref, keys, vals
):
    step = pl.program_id(0)
    width, window = k_ref.shape[0], q_ref.shape[0]
    heads = q_ref.shape[1] // width

    @pl.when(step == 0)
    def _():
        def scaled_columns(data):
            wide = data.astype(jnp.float32)
            scale = lax.rsqrt(jnp.mean(wide * wide, axis=0, keepdims=True) + EPS)
            return (wide * scale * kg_ref[...]).astype(jnp.bfloat16)

        keys[:, :window] = scaled_columns(halo_ref[:width, :])
        keys[:, window:] = scaled_columns(k_ref[...])
        vals[:, :window] = halo_ref[width:, :]
        vals[:, window:] = v_ref[...]

    span = pl.ds(pl.multiple_of(step * window, window), 2 * window)
    part = [scaled_rows(q_ref[:, h * width : (h + 1) * width], qg_ref[...]) for h in range(heads)]
    scores = jnp.dot(
        jnp.concatenate(part, axis=0), keys[:, span], preferred_element_type=jnp.float32
    ) * width ** (-0.5)
    shape = (window, 2 * window)
    column = lax.broadcasted_iota(jnp.int32, shape, 1)
    lag = window + lax.broadcasted_iota(jnp.int32, shape, 0) - column
    starts = (step > 0) | (place_ref[0] > 0)
    valid = (lag >= 0) & (lag < window) & ((column >= window) | starts)
    weights = []
    for h in range(heads):
        sink = sink_ref[h]
        score = jnp.where(valid, scores[h * window : (h + 1) * window], -1e30)
        peak = jnp.maximum(jnp.max(score, axis=-1, keepdims=True), sink)
        terms = jnp.exp(score - peak)
        total = jnp.sum(terms, axis=-1, keepdims=True) + jnp.exp(sink - peak)
        weights.append((terms / total).astype(jnp.bfloat16))
    mixed = lax.dot_general(
        jnp.concatenate(weights, axis=0),
        vals[:, span],
        (((1,), (1,)), ((), ())),
        preferred_element_type=jnp.float32,
    ).astype(jnp.bfloat16)
    out_ref[...] = jnp.concatenate(
        [mixed[h * window : (h + 1) * window] for h in range(heads)], axis=1
    )


def attend(place, sinks, queries, keys, values, halo, query_gain, key_gain):
    width, rows = keys.shape
    window = WINDOW
    full = lambda a: pl.BlockSpec(a.shape, lambda i, p, s: (0,) * a.ndim)
    row_spec = pl.BlockSpec((window, queries.shape[1]), lambda i, p, s: (i, 0))
    gains = (query_gain[None], key_gain[:, None])
    return pl.pallas_call(
        attend_kernel,
        grid_spec=pltpu.PrefetchScalarGridSpec(
            num_scalar_prefetch=2,
            grid=(rows // window,),
            in_specs=[row_spec, full(keys), full(values), full(halo), *map(full, gains)],
            out_specs=row_spec,
            scratch_shapes=[pltpu.VMEM((width, rows + window), jnp.bfloat16)] * 2,
        ),
        out_shape=jax.ShapeDtypeStruct(queries.shape, jnp.bfloat16),
        cost_estimate=pl.CostEstimate(
            flops=rows * window * width * 400, bytes_accessed=rows * 1024, transcendentals=0
        ),
        name="attend",
    )(place, sinks, queries, keys, values, halo, *gains)


def halves_kernel(main, tail, place_ref, gate_ref, up_ref, *outs):
    def put(refs, h):
        start = 0
        for ref in refs:
            rows = slice(start, start + ref.shape[0])
            start += ref.shape[0]
            ref[:, :main] = gate_ref[rows, h * main : (h + 1) * main]
            ref[:, main : 2 * main] = up_ref[rows, h * main : (h + 1) * main]
            if tail:
                rest = [r[rows, 2 * main :][:, h * tail :][:, :tail] for r in (gate_ref, up_ref)]
                ref[:, 2 * main :] = jnp.concatenate(rest, axis=1)

    for low in (0, 1):

        @pl.when(place_ref[0] == low)
        def _():
            put(outs[:1], low)
            put(outs[1:], 1 - low)


def down_halves_kernel(main, tail, place_ref, down_ref, own_ref, far_ref):
    def put(ref, h):
        ref[:main, :] = down_ref[h * main : (h + 1) * main, :]
        if tail:
            ref[main:, :] = down_ref[2 * main + h * tail : 2 * main + (h + 1) * tail, :]

    for low in (0, 1):

        @pl.when(place_ref[0] == low)
        def _():
            put(own_ref, low)
            put(far_ref, 1 - low)


def split(kernel, place, shapes, *weights):
    spec = lambda s: pl.BlockSpec(s, lambda i, p: (0, 0))
    return pl.pallas_call(
        kernel,
        grid_spec=pltpu.PrefetchScalarGridSpec(
            num_scalar_prefetch=1,
            grid=(1,),
            in_specs=[spec(w.shape) for w in weights],
            out_specs=[spec(s) for s in shapes],
        ),
        out_shape=[jax.ShapeDtypeStruct(s, jnp.bfloat16) for s in shapes],
        cost_estimate=pl.CostEstimate(flops=10**9, bytes_accessed=10**6, transcendentals=0),
    )(place, *weights)


def normed_rows(columns, atts, outs, ress, gains, held, normed_ref):
    width = ress[0].shape[1]
    squares = 0.0
    for n in range(4):
        total = sum(
            jnp.dot(a[...], o[:, columns[n]], preferred_element_type=jnp.float32)
            for a, o in zip(atts, outs)
        )
        middle = (total + ress[n][...].astype(jnp.float32)).astype(jnp.bfloat16)
        wide = middle.astype(jnp.float32)
        squares += jnp.sum(wide * wide, axis=1, keepdims=True)
        held[n] = middle
    scale = lax.rsqrt(squares / (4 * width) + EPS)
    for n in range(4):
        wide = held[n].astype(jnp.float32)
        normed_ref[:, columns[n]] = (wide * scale * gains[n][...]).astype(jnp.bfloat16)


def spans(place_ref, first, count, width):
    return [
        pl.ds(pl.multiple_of(place_ref[first + n] * width, width), width) for n in range(count)
    ]


def project_kernel(place_ref, *refs):
    atts, outs, ress, gains = (refs[4 * n : 4 * n + 4] for n in range(4))
    normed_ref, middle_ref, held = refs[16:]
    columns = spans(place_ref, 0, 4, ress[0].shape[1])
    normed_rows(columns, atts, outs, ress, gains, held, normed_ref)
    middle_ref[...] = held[0]


def project(place, atts, outs, ress, gains, tile):
    rows, depth = atts[0].shape
    width = outs[0].shape[1]
    part = ress[0].shape[1]
    row_spec = lambda n: pl.BlockSpec((tile, n), lambda i, p: (i, 0))
    full_spec = lambda a: pl.BlockSpec(a.shape, lambda i, p: (0, 0))
    return pl.pallas_call(
        project_kernel,
        grid_spec=pltpu.PrefetchScalarGridSpec(
            num_scalar_prefetch=1,
            grid=(rows // tile,),
            in_specs=[row_spec(depth)] * 4
            + [full_spec(o) for o in outs]
            + [row_spec(part)] * 4
            + [full_spec(g) for g in gains],
            out_specs=[row_spec(width), row_spec(part)],
            scratch_shapes=[pltpu.VMEM((4, tile, part), jnp.bfloat16)],
        ),
        out_shape=[
            jax.ShapeDtypeStruct((rows, width), jnp.bfloat16),
            jax.ShapeDtypeStruct((rows, part), jnp.bfloat16),
        ],
        compiler_params=pltpu.CompilerParams(vmem_limit_bytes=PROJECT_MIB * MIB),
        cost_estimate=pl.CostEstimate(
            flops=8 * rows * depth * width, bytes_accessed=4 * rows * width, transcendentals=0
        ),
    )(place, *atts, *outs, *ress, *gains)


def stack_pieces(pieces, whole):
    start = 0
    for piece in pieces:
        whole[start : start + piece.shape[0], :] = piece[...]
        start += piece.shape[0]


def put_hidden(main, tail, acts, out_ref):
    def gated(gate, up):
        return (gate / (1.0 + jnp.exp(-gate)) * up).astype(jnp.bfloat16)

    out_ref[:, :main] = gated(acts[:, :main], acts[:, main : 2 * main])
    if tail:
        rest = acts[:, 2 * main :]
        out_ref[:, main:] = gated(rest[:, :tail], rest[:, tail:])


def product(columns, x_ref, whole):
    x = jnp.concatenate([x_ref[:, c] for c in columns], axis=1)
    return jnp.dot(x, whole[...], preferred_element_type=jnp.float32)


def far_kernel(main, tail, count, place_ref, *refs):
    atts, outs, ress, gains = (refs[4 * n : 4 * n + 4] for n in range(4))
    pieces, (out_ref, whole, held, x_ref) = refs[16 : 16 + count], refs[16 + count :]
    pl.when(pl.program_id(0) == 0)(lambda: stack_pieces(pieces, whole))
    columns = spans(place_ref, 0, 4, ress[0].shape[1])
    normed_rows(columns, atts, outs, ress, gains, held, x_ref)
    acts = product(spans(place_ref, 4, 8, x_ref.shape[1] // 8), x_ref, whole)
    put_hidden(main, tail, acts, out_ref)


def far_hidden(place, atts, outs, ress, gains, pieces, main, tail, tile):
    rows, part = ress[0].shape
    depth = sum(p.shape[0] for p in pieces)
    width = pieces[0].shape[1]
    tiles = rows // tile
    row_spec = lambda a: pl.BlockSpec((tile, a.shape[1]), lambda i, p: (i, 0))
    full = lambda a: pl.BlockSpec(a.shape, lambda i, p: (0, 0), pipeline_mode=pl.Buffered(1))
    operands = [*atts, *outs, *ress, *gains, *pieces]
    specs = [*map(row_spec, atts), *map(full, outs), *map(row_spec, ress)]
    return pl.pallas_call(
        functools.partial(far_kernel, main, tail, len(pieces)),
        grid_spec=pltpu.PrefetchScalarGridSpec(
            num_scalar_prefetch=1,
            grid=(tiles,),
            in_specs=[*specs, *map(full, [*gains, *pieces])],
            out_specs=pl.BlockSpec((tile, main + tail), lambda i, p: (i, 0)),
            scratch_shapes=[
                pltpu.VMEM((depth, width), jnp.bfloat16),
                pltpu.VMEM((4, tile, part), jnp.bfloat16),
                pltpu.VMEM((tile, depth), jnp.bfloat16),
            ],
        ),
        out_shape=jax.ShapeDtypeStruct((rows, main + tail), jnp.bfloat16),
        compiler_params=pltpu.CompilerParams(vmem_limit_bytes=HIDDEN_MIB * MIB),
        cost_estimate=pl.CostEstimate(
            flops=4 * rows * depth * width, bytes_accessed=8 * rows * width, transcendentals=0
        ),
        name="far_hidden",
    )(place, *operands)


def partial_kernel(count, place_ref, x_ref, *refs):
    pieces, out_ref, whole = refs[:count], refs[count], refs[count + 1]
    pl.when(pl.program_id(0) == 0)(lambda: stack_pieces(pieces, whole))
    depth = x_ref.shape[1] // 8
    columns = spans(place_ref, 4, whole.shape[0] // depth, depth)
    out_ref[...] = product(columns, x_ref, whole)


def near_kernel(main, tail, count, place_ref, x_ref, acts_ref, *refs):
    pieces, (out_ref, whole) = refs[:count], refs[count:]
    pl.when(pl.program_id(0) == 0)(lambda: stack_pieces(pieces, whole))
    depth = x_ref.shape[1] // 8
    blocks = whole.shape[0] // depth
    columns = spans(place_ref, 12 - blocks, blocks, depth)
    put_hidden(main, tail, acts_ref[...] + product(columns, x_ref, whole), out_ref)


def near_step(kernel, place, x, more, pieces, out_shape, limit, tile):
    rows, _ = x.shape
    total = sum(p.shape[0] for p in pieces)
    row_spec = lambda a: pl.BlockSpec((tile, a.shape[1]), lambda i, p: (i, 0))
    full = lambda a: pl.BlockSpec(a.shape, lambda i, p: (0, 0), pipeline_mode=pl.Buffered(1))
    return pl.pallas_call(
        kernel,
        grid_spec=pltpu.PrefetchScalarGridSpec(
            num_scalar_prefetch=1,
            grid=(rows // tile,),
            in_specs=[row_spec(x), *map(row_spec, more), *map(full, pieces)],
            out_specs=row_spec(out_shape),
            scratch_shapes=[pltpu.VMEM((total, pieces[0].shape[1]), jnp.bfloat16)],
        ),
        out_shape=out_shape,
        compiler_params=pltpu.CompilerParams(vmem_limit_bytes=limit * MIB),
        cost_estimate=pl.CostEstimate(
            flops=3000 * rows * total, bytes_accessed=4000 * rows, transcendentals=0
        ),
    )(place, x, *more, *pieces)


def down_kernel(kept, flag_ref, near_ref, far_ref, *refs):
    pieces, (*got_ref, out_ref, whole) = refs[:4], refs[4:]
    block = pieces[0].shape[1]

    @pl.when(pl.program_id(0) == 0)
    def _():
        for same in (0, 1):
            for near in (0, 1):

                @pl.when((flag_ref[0] == same) & (flag_ref[1] == near))
                def _():
                    for n, piece in enumerate(pieces):
                        if ((n % 2) != same) == kept:
                            at = block if (n // 2) == near else 0
                            whole[:, at : at + block] = piece[...]

    def put(hidden_ref):
        acts = jnp.dot(hidden_ref[...], whole[...], preferred_element_type=jnp.float32)
        if kept:
            acts += got_ref[0][...].astype(jnp.float32)
        out_ref[...] = acts.astype(jnp.bfloat16)

    pl.when(pl.program_id(0) == 0)(lambda: put(near_ref))
    pl.when(pl.program_id(0) == 1)(lambda: put(far_ref))


def down(flags, near, far, pieces, got=()):
    rows, depth = near.shape
    block = pieces[0].shape[1]
    row_spec = pl.BlockSpec((rows, 2 * block), lambda i, p: (i, 0))
    full = lambda a: pl.BlockSpec(a.shape, lambda i, p: (0, 0))
    return pl.pallas_call(
        functools.partial(down_kernel, bool(got)),
        grid_spec=pltpu.PrefetchScalarGridSpec(
            num_scalar_prefetch=1,
            grid=(2,),
            in_specs=[full(near), full(far), *map(full, pieces)] + [row_spec] * len(got),
            out_specs=row_spec,
            scratch_shapes=[pltpu.VMEM((depth, 2 * block), jnp.bfloat16)],
        ),
        out_shape=jax.ShapeDtypeStruct((2 * rows, 2 * block), jnp.bfloat16),
        compiler_params=pltpu.CompilerParams(vmem_limit_bytes=DOWN_MIB * MIB),
        cost_estimate=pl.CostEstimate(
            flops=8 * rows * depth * block, bytes_accessed=8 * rows * block, transcendentals=0
        ),
    )(flags, near, far, *pieces, *got)


def finish_kernel(flag_ref, middle_ref, ahead_ref, ahead_got, behind_ref, behind_got, out_ref):
    block = ahead_ref.shape[1]
    pairs = ((ahead_ref, ahead_got), (behind_ref, behind_got))
    for odd in (0, 1):

        @pl.when(flag_ref[0] == odd)
        def _():
            for n, (kept, got) in enumerate(pairs):
                columns = slice((n ^ odd) * block, ((n ^ odd) + 1) * block)
                feed = kept[...].astype(jnp.float32) + got[...].astype(jnp.float32)
                total = middle_ref[:, columns].astype(jnp.float32) + 0.5 * feed
                out_ref[:, columns] = total.astype(jnp.bfloat16)


def finish(flag, middle, ahead, ahead_got, behind, behind_got):
    rows, width = middle.shape
    block = ahead.shape[1]
    tile = rows // 2
    wide = pl.BlockSpec((tile, width), lambda i, p: (i, 0))
    half = pl.BlockSpec((tile, block), lambda i, p: (i, 0))
    return pl.pallas_call(
        finish_kernel,
        grid_spec=pltpu.PrefetchScalarGridSpec(
            num_scalar_prefetch=1,
            grid=(2,),
            in_specs=[wide, half, half, half, half],
            out_specs=wide,
        ),
        out_shape=jax.ShapeDtypeStruct((rows, width), jnp.bfloat16),
        cost_estimate=pl.CostEstimate(
            flops=rows * width * 8, bytes_accessed=rows * width * 8, transcendentals=0
        ),
        name="finish",
    )(flag, middle, ahead, ahead_got, behind, behind_got)


def paired_device(
    queries, keys, values, query_gain, key_gain, sink_logits, out_weight, residual, norm_gain,
    gate_weight, up_weight, down_weight,
):
    zh, zl, y, x, c = (lax.axis_index(a) for a in ("zh", "zl", "y", "x", "c"))
    rows = queries.shape[0]
    block = down_weight.shape[1]
    units = gate_weight.shape[1]
    main = units // LANES // 2 * LANES
    tail = (units - 2 * main) // 2
    one = lambda v: v.astype(jnp.int32).reshape(1)

    sp_axes = ("zh", "zl", "y")
    keys, values = keys.T, values.T
    edge = jnp.concatenate([keys[:, rows - WINDOW :], values[:, rows - WINDOW :]], axis=0)
    halo = from_behind(edge, sp_axes, lax.axis_size(sp_axes))

    depth = gate_weight.shape[0]
    gu_own, *gu_far = split(
        functools.partial(halves_kernel, main, tail), one(zl),
        [(depth, units), (depth // 2, units), (depth // 2, units)], gate_weight, up_weight,
    )
    pair = lambda parts, axis: [swap(parts[n], axis) for n in (0, 1)]
    gu_swp = pair(gu_far, "zl")
    gu_own_m = swap(gu_own, "zh")
    gu_own_y = swap(gu_own, "y")
    res2 = swap(residual, "zl")
    dn_own, dn_far = split(
        functools.partial(down_halves_kernel, main, tail), one(zl),
        [(main + tail, block)] * 2, down_weight,
    )
    attended = attend(
        one(lax.axis_index(sp_axes)), sink_logits, queries, keys, values, halo, query_gain,
        key_gain,
    )
    att2 = swap(attended, "zl")
    gu_swp_m = pair(gu_swp, "zh")
    gu_swp_y = pair(gu_swp, "y")
    dn_swp = swap(dn_far, "zl")
    dn_own_m = swap(dn_own, "zh")
    dn_own_y = swap(dn_own, "y")
    gu_own_my = swap(gu_own_m, "y")

    place = jnp.stack(
        [2 * x + c, 2 * (1 - x) + c, 2 * x + (1 - c), 2 * (1 - x) + (1 - c)]
    ).astype(jnp.int32)

    def over_tp(own):
        far = swap(own, "x")
        return own, far, swap(own, "c"), swap(far, "c")

    gains = over_tp(norm_gain[None])
    rest = out_weight.shape[0] // 2
    mine = swap(lax.dynamic_slice_in_dim(out_weight, y * rest, rest), "x")
    theirs = swap(mine, "y")
    out_x = jnp.concatenate(
        [jnp.where(y == 0, mine, theirs), jnp.where(y == 0, theirs, mine)], axis=0
    )
    outs = out_weight, out_x, swap(out_weight, "c"), swap(out_x, "c")
    normed, middle = project(
        place, over_tp(attended), outs, over_tp(residual), gains,
        rows // 2,
    )
    att2s, res2s = over_tp(att2), over_tp(res2)

    gu_swp_my = pair(gu_swp_m, "y")
    dn_swp_m = swap(dn_swp, "zh")
    dn_swp_y = swap(dn_swp, "y")
    dn_own_my = swap(dn_own_m, "y")
    dn_swp_my = swap(dn_swp_m, "y")

    pieces = [gu_own, gu_own_y, *gu_swp, *gu_swp_y, gu_own_m, gu_own_my]
    at = lambda n: 4 * (zh ^ (n // 4)) + 2 * (zl ^ (n // 2 % 2)) + (y ^ (n % 2))
    spots = jnp.stack([at(n) for n in range(8)]).astype(jnp.int32)
    last = [*gu_swp_m, *gu_swp_my]
    where = jnp.concatenate([place, spots])
    acts = near_step(
        functools.partial(partial_kernel, len(pieces)), where, normed, (), pieces,
        jax.ShapeDtypeStruct((rows, units), jnp.float32), PARTIAL_MIB, rows // 2,
    )
    near = near_step(
        functools.partial(near_kernel, main, tail, len(last)), where, normed,
        (acts,), last, jax.ShapeDtypeStruct((rows, main + tail), jnp.bfloat16), NEAR_MIB,
        rows // 2,
    )
    pieces += last
    far = far_hidden(where, att2s, outs, res2s, gains, pieces, main, tail, rows)

    flags = jnp.stack([c == zl, x == zh]).astype(jnp.int32)
    wide = lambda v: v.astype(jnp.float32)
    add = lambda a, b: wide(a) + wide(b)

    def reduced(pieces, rows_first):
        sent = down(flags, near, far, pieces)
        got = swap(sent, "c")
        total = down(flags, near, far, pieces, (got,))
        if rows_first:
            got = swap(total[rows:], "zl")
            total = add(total[:rows], got).astype(jnp.bfloat16)
            return total[:, :block], swap(total[:, block:], "x")
        got = swap(total[:, block:], "x")
        total = add(total[:, :block], got).astype(jnp.bfloat16)
        return total[:rows], swap(total[rows:], "zl")

    ahead = reduced((dn_own, dn_swp, dn_own_m, dn_swp_m), True)
    behind = reduced((dn_own_y, dn_swp_y, dn_own_my, dn_swp_my), False)
    return finish(one(y), middle, *ahead, *behind)


def solution(mesh):
    sp, tp = mesh.shape["sp"], mesh.shape["tp"]

    def spread(fine, sp_axes, tp_axes, body):
        both = P(sp_axes, tp_axes)
        heads, rows = P(tp_axes), P(tp_axes, None)
        in_specs = (both, both, both, P(), P(), heads, rows, both, heads, both, both)
        return jax.shard_map(
            body,
            mesh=fine,
            in_specs=(*in_specs, P(tp_axes, sp_axes)),
            out_specs=both,
            check_vma=False,
        )

    def step(*args):
        if (sp, tp) == (8, 4) and args[1].shape[1] == tp * args[3].shape[0]:
            fine = Mesh(mesh.devices.reshape(2, 2, 2, 2, 2), ("zh", "zl", "y", "x", "c"))
            return spread(fine, ("zh", "zl", "y"), ("x", "c"), paired_device)(*args)
        body = functools.partial(general_device, args[8].shape[0])
        return spread(mesh, "sp", "tp", body)(*args)

    return step
```
